256 devices in a mesh: ep: 16 (over y, x), tp: 16 (over z, core).
Axes of the slice: x: 4, y: 4, z: 8, core: 2. Of those that a mesh axis runs over, the one named last changes fastest.
Arguments:
- mixer_input_rows: bfloat16 [32768, 2048], P(('ep', 'tp')), may hold values from -6 to 6
- mixer_norm_gain: float32 [2048], replicated, may hold values from 0.1 to 1.9
- query_weight: bfloat16 [2048, 2048], P(None, 'tp'), may hold values from -0.125 to 0.125
- key_weight: bfloat16 [2048, 2048], P(None, 'tp'), may hold values from -0.125 to 0.125
- value_weight: bfloat16 [2048, 2048], P(None, 'tp'), may hold values from -0.125 to 0.125
- write_strength_projection: bfloat16 [2048, 16], replicated, may hold values from -0.125 to 0.125
- decay_projection: bfloat16 [2048, 16], replicated, may hold values from -0.125 to 0.125
- head_decay_speed: float32 [16], P('tp'), may hold values from 0 to 1
- largest_write_strength: float32 [16], P('tp'), may hold values from 0 to 1
- extra_log_decay: float32 [32768, 16], P('ep', 'tp'), may hold values from -1 to 0
- head_norm_gain: float32 [128], replicated, may hold values from 0.1 to 1.9
- mixer_output_weight: bfloat16 [2048, 2048], P('tp'), may hold values from -0.125 to 0.125
- expert_input_rows: bfloat16 [2048, 2048], P(('ep', 'tp')), may hold values from -6 to 6
- expert_norm_gain: float32 [2048], replicated, may hold values from 0.1 to 1.9
- routes: int32 [2048, 2], P(('ep', 'tp')), may hold values from 0 to 15, all different within a row; in each aligned block of 8 rows (0 to 7, 8 to 15, ...) at most 2 rows name the same one
- expert_route_weight: float32 [2048, 2], P(('ep', 'tp')), may hold values from 0.2 to 1
- gate_weight: bfloat16 [16, 2048, 7168], P('ep', None, 'tp'), may hold values from -0.125 to 0.125
- up_weight: bfloat16 [16, 2048, 7168], P('ep', None, 'tp'), may hold values from -0.125 to 0.125
- down_weight: bfloat16 [16, 7168, 2048], P('ep', 'tp'), may hold values from -0.0625 to 0.0625
Outputs:
- mix_out: bfloat16 [32768, 2048], P(('ep', 'tp'))
- exp_out: bfloat16 [2048, 2048], P(('ep', 'tp'))
The draws below stay inside these ranges and needn't reach their ends.
Inputs may be any that keep to these rules, and one draw needn't show every extreme that they name: `routes`: within the rows of one device (aligned blocks of 8 rows) no expert is named more than 2 times, some device names some expert exactly 2 times, and the 2 experts of a row differ.
All inputs are finite; a program needn't handle non-finite values.
Results may differ from the reference program's by a relative error of at most 0.019.
Values may be sent and summed in bfloat16 or wider, within the bound.
No kernel may reach another device: no remote copies, remote signals or barrier semaphores. Data moves between devices by JAX's collectives and lax.ppermute only.
A program may use at most 128 MiB of HBM per device.

```python
import math
import jax
import jax.numpy as jnp
import numpy as np
from jax import lax

D = 2048
HEADS = 16
HEAD = 128
FF = 7168
BLOCK = 128
TOP = 2
EXP_TOK_DEV = 8
HEADS_DEV = 1
FF_DEV = 448
SPAN_EP = 2048
SEQ = 32768
EXP_TOKENS = 2048
EXPERTS = 16
CAP = 2
N_EP = 16
N_TP = 16


def head_split(key):
    ranks = jax.random.permutation(jax.random.fold_in(key, 101), HEADS)
    quick_count = HEADS // 2
    return ranks < quick_count


def draw_head_decay_speed(key, part):
    quick = head_split(key)
    fast_rate = jax.random.uniform(jax.random.fold_in(key, 102), (HEADS,), jnp.float32, 0.025, 0.05)
    slow_rate = jax.random.uniform(jax.random.fold_in(key, 103), (HEADS,), jnp.float32, 0.1, 0.3) / SEQ
    return jnp.where(quick, fast_rate, slow_rate)


def draw_largest_write_strength(key, part):
    quick = head_split(key)
    fast_rate = jax.random.uniform(jax.random.fold_in(key, 104), (HEADS,), jnp.float32, 0.6, 1.0)
    slow_rate = jax.random.uniform(jax.random.fold_in(key, 105), (HEADS,), jnp.float32, 0.5, 1.0) * HEAD / SEQ
    return jnp.where(quick, fast_rate, slow_rate)


def draw_extra_log_decay(key, part):
    span_count = SEQ // SPAN_EP
    position = jnp.arange(SEQ)
    steady = jax.random.uniform(jax.random.fold_in(key, 111), (span_count, HEADS), jnp.float32, 0.12, 0.5)
    level = -steady[position // SPAN_EP] / SEQ
    spots = jax.random.randint(jax.random.fold_in(key, 112), (3,), 0, SEQ)
    drops = jnp.log(jax.random.uniform(jax.random.fold_in(key, 113), (3, HEADS), jnp.float32, 0.6, 0.8))
    hits = (position[:, None] == spots[None, :]).astype(jnp.float32)
    return level + jnp.sum(hits[:, :, None] * drops[None, :, :], axis=1)


def shard_levels(own_key, extent, shards, smallest, top_value):
    factor_of, own = 1.0, jax.random.fold_in(own_key, 6)
    for dim, shards_of in shards:
        steps = jnp.exp(jax.random.uniform(jax.random.fold_in(own, dim), (shards_of,), jnp.float32, smallest / len(shards), top_value / len(shards)))
        factor_of = factor_of * jnp.repeat(steps, extent[dim] // shards_of).reshape([-1 if axis == dim else 1 for axis in range(len(extent))])
    return factor_of


def routed_block(stream_key, own, number, rows, count, top, limit, slope):
    order = jax.random.permutation(stream_key, count)
    packed, common = load_shares(count, rows * top, limit, slope, True), load_shares(count, rows * top, limit, slope, False)
    places = jnp.arange(count)

    def named(tallies, offset_by):
        used = int((tallies > 0).sum())
        fixed = max(1, used // 4)
        passed = fixed + (places - fixed + offset_by * (used - fixed)) % max(1, count - fixed)
        return jnp.zeros((count,), jnp.int32).at[order[jnp.where(places < fixed, places, passed)]].set(jnp.asarray(tallies, jnp.int32))

    tallies = jnp.where(number % 4 == 0, named(packed, number // 4), named(common, number - number // 4 - 1))
    mixed = jax.random.permutation(jax.random.fold_in(own, 3), count)
    source_of, taker = mixed[0:count // 2 * 2:2], mixed[1:count // 2 * 2:2]
    margin = jnp.minimum(tallies[source_of] - 1, limit - tallies[taker]) // 2
    margin = jnp.where((source_of == order[0]) | (taker == order[0]) | (tallies[taker] == 0), 0, jnp.maximum(margin, 0))
    passed = jax.random.randint(jax.random.fold_in(own, 4), (count // 2,), 0, 1 << 20) % (margin + 1)
    tallies = tallies.at[source_of].add(-passed).at[taker].add(passed)
    members = jnp.searchsorted(jnp.cumsum(tallies), jnp.arange(rows * top), side="right").astype(jnp.int32)
    listing = members.reshape(top, rows).T
    listing = listing[jax.random.permutation(jax.random.fold_in(own, 1), rows)]
    offset_by = jax.random.randint(jax.random.fold_in(own, 2), (rows, 1), 0, top)
    return jnp.take_along_axis(listing, (jnp.arange(top)[None, :] + offset_by) % top, axis=1)


def load_shares(number_of, total, reach, lean, full):
    portions = [(1 << 20) // math.isqrt(rank ** lean) + 1 for rank in range(1, number_of + 1)]
    largest = reach if full else min(reach, max(-(-total // number_of), total * portions[0] // sum(portions)))
    least = 1 if total - largest >= number_of - 1 else 0
    counts, spare = [largest] + [least] * (number_of - 1), total - largest - least * (number_of - 1)
    while spare > 0:
        free = [i for i in range(1, number_of) if counts[i] < largest] or [i for i in range(1, number_of) if counts[i] < reach]
        pool, remaining = sum([portions[i] for i in free]), spare
        for i in free:
            more = min(reach - counts[i], max(1, remaining * portions[i] // pool), spare)
            counts[i] = counts[i] + more
            spare = spare - more
    return np.array(counts)


def scatter_about(own_key, extent, scale, bound, cuts=(), kind=jnp.bfloat16):
    level = shard_levels(own_key, extent, cuts, -0.22, 0.18) if cuts else 1.0
    array = jax.random.normal(own_key, extent, jnp.float32) * scale * level
    return jnp.minimum(jnp.maximum(array, -bound), bound).astype(kind)


def setup_inputs(seed: int = 0) -> dict:
    streams_of = jax.random.split(jax.random.key(seed), 20)
    mixer_input_rows = scatter_about(streams_of[0], (SEQ, D), 1.0, 6.0, ((0, 256),))
    mixer_norm_gain = jnp.clip(1.0 + 0.18 * jax.random.normal(streams_of[1], (D,), jnp.float32), 0.1, 1.9)
    query_weight = scatter_about(streams_of[2], (D, HEADS * HEAD), D ** -0.5, 0.125, ((1, 16),))
    key_weight = scatter_about(streams_of[3], (D, HEADS * HEAD), D ** -0.5, 0.125, ((1, 16),))
    value_weight = scatter_about(streams_of[4], (D, HEADS * HEAD), D ** -0.5, 0.125, ((1, 16),))
    write_strength_projection = scatter_about(streams_of[5], (D, HEADS), D ** -0.5, 0.125)
    decay_projection = scatter_about(streams_of[6], (D, HEADS), D ** -0.5, 0.125)
    head_decay_speed = draw_head_decay_speed(jax.random.fold_in(streams_of[19], 71), 0)
    largest_write_strength = draw_largest_write_strength(jax.random.fold_in(streams_of[19], 71), 0)
    extra_log_decay = draw_extra_log_decay(jax.random.fold_in(streams_of[19], 71), 0)
    head_norm_gain = jnp.clip(1.0 + 0.18 * jax.random.normal(streams_of[10], (HEAD,), jnp.float32), 0.1, 1.9)
    mixer_output_weight = scatter_about(streams_of[11], (HEADS * HEAD, D), (HEADS * HEAD) ** -0.5, 0.125, ((0, 16),))
    expert_input_rows = scatter_about(streams_of[12], (EXP_TOKENS, D), 1.0, 6.0, ((0, 256),))
    expert_norm_gain = jnp.clip(1.0 + 0.18 * jax.random.normal(streams_of[13], (D,), jnp.float32), 0.1, 1.9)
    routes_keys = jax.random.split(jax.random.fold_in(streams_of[14], 1), EXP_TOKENS // EXP_TOK_DEV)
    routes_turns = jax.random.permutation(jax.random.fold_in(streams_of[14], 3), EXP_TOKENS // EXP_TOK_DEV)
    routes = jax.vmap(lambda own, number: routed_block(jax.random.fold_in(streams_of[14], 2), own, number, EXP_TOK_DEV, EXPERTS, TOP, CAP, 2))(routes_keys, routes_turns).reshape((EXP_TOKENS, TOP))
    expert_route_weight = jnp.clip(0.2 + 0.8 * jax.random.uniform(streams_of[15], (EXP_TOKENS, TOP), jnp.float32) ** shard_levels(streams_of[15], (EXP_TOKENS, TOP), ((0, 256),), -0.2, 0.2), 0.2, 1.0)
    gate_weight = scatter_about(streams_of[16], (EXPERTS, D, FF), D ** -0.5, 0.125, ((0, 16), (2, 16)))
    up_weight = scatter_about(streams_of[17], (EXPERTS, D, FF), D ** -0.5, 0.125, ((0, 16), (2, 16)))
    down_weight = scatter_about(streams_of[18], (EXPERTS, FF, D), FF ** -0.5, 0.0625, ((0, 16), (1, 16)))
    return {"mixer_input_rows": mixer_input_rows, "mixer_norm_gain": mixer_norm_gain, "query_weight": query_weight, "key_weight": key_weight, "value_weight": value_weight, "write_strength_projection": write_strength_projection, "decay_projection": decay_projection, "head_decay_speed": head_decay_speed, "largest_write_strength": largest_write_strength, "extra_log_decay": extra_log_decay, "head_norm_gain": head_norm_gain, "mixer_output_weight": mixer_output_weight, "expert_input_rows": expert_input_rows, "expert_norm_gain": expert_norm_gain, "routes": routes, "expert_route_weight": expert_route_weight, "gate_weight": gate_weight, "up_weight": up_weight, "down_weight": down_weight}


norm_eps = 1e-06
highest = lax.Precision.HIGHEST

def rms_scale(rows_in, gain_vec):
    widened = rows_in.astype(jnp.float32)
    scaled = widened * lax.rsqrt(lax.optimization_barrier(jnp.mean(widened * widened, axis=-1, keepdims=True)) + norm_eps)
    return (scaled * gain_vec).astype(jnp.bfloat16)

def unit_rows(tensor):
    return tensor * lax.rsqrt(lax.optimization_barrier(jnp.sum(tensor * tensor, axis=-1, keepdims=True)) + 1e-06)

def block_terms(queries, key_rows, values, log_decay_values, strength):
    length = log_decay_values.shape[-1]
    cumulative = jnp.cumsum(log_decay_values, axis=-1)
    causal = jnp.tril(jnp.ones((length, length), jnp.bool_))
    strict = jnp.tril(jnp.ones((length, length), jnp.bool_), -1)
    decays = jnp.exp(jnp.where(causal, cumulative[..., :, None] - cumulative[..., None, :], -jnp.inf))
    keys_scaled = key_rows * strength[..., None]
    inner_prod = jnp.einsum('...cd,...sd->...cs', keys_scaled, key_rows, precision=highest)
    system = jnp.where(strict, inner_prod * decays, 0.0) + jnp.eye(length, dtype=key_rows.dtype)
    right_side = jnp.concatenate([values * strength[..., None], keys_scaled * jnp.exp(cumulative)[..., None]], axis=-1)
    solved = jax.scipy.linalg.solve_triangular(system, right_side, lower=True, unit_diagonal=True)
    value_width = values.shape[-1]
    carried = solved[..., :value_width]
    weights = solved[..., value_width:]
    scores = jnp.einsum('...cd,...sd->...cs', queries, key_rows, precision=highest) * decays
    query_dec = queries * jnp.exp(cumulative)[..., None]
    keys_dec = key_rows * jnp.exp(cumulative[..., -1:] - cumulative)[..., None]
    last_decay = jnp.exp(cumulative[..., -1])
    return (carried, weights, scores, query_dec, keys_dec, last_decay)

def apply_block(memory, carried, weights, scores, query_dec, keys_dec, last_decay):
    fresh_values = carried - jnp.einsum('...cd,...de->...ce', weights, memory, precision=highest)
    output = jnp.einsum('...cd,...de->...ce', query_dec, memory, precision=highest)
    output = output + jnp.einsum('...cs,...se->...ce', scores, fresh_values, precision=highest)
    memory = memory * last_decay[..., None, None] + jnp.einsum('...cd,...ce->...de', keys_dec, fresh_values, precision=highest)
    return (memory, output)

def reference(mixer_input_rows, mixer_norm_gain, query_weight, key_weight, value_weight, write_strength_projection, decay_projection, head_decay_speed, largest_write_strength, extra_log_decay, head_norm_gain, mixer_output_weight, expert_input_rows, expert_norm_gain, routes, expert_route_weight, gate_weight, up_weight, down_weight):
    mix_normed = rms_scale(mixer_input_rows, mixer_norm_gain)

    def apply_projection(weight):
        return jnp.dot(mix_normed.astype(jnp.float32), weight.astype(jnp.float32), preferred_element_type=jnp.float32)
    queries = jax.nn.silu(apply_projection(query_weight)).reshape(SEQ, HEADS, HEAD)
    key_rows = unit_rows(jax.nn.silu(apply_projection(key_weight)).reshape(SEQ, HEADS, HEAD))
    values = jax.nn.silu(apply_projection(value_weight)).reshape(SEQ, HEADS, HEAD)
    strength = largest_write_strength * jax.nn.sigmoid(apply_projection(write_strength_projection))
    log_decay_values = extra_log_decay - head_decay_speed * jax.nn.softplus(apply_projection(decay_projection))
    block_count = SEQ // BLOCK

    def blocked(tensor):
        return tensor.reshape(block_count, BLOCK, HEADS, -1).transpose(0, 2, 1, 3)

    def advance(memory, pieces):
        return apply_block(memory, *block_terms(*pieces))
    initial = jnp.zeros((HEADS, HEAD, HEAD), jnp.float32)
    _, outputs = lax.scan(advance, initial, (blocked(queries), blocked(key_rows), blocked(values), blocked(log_decay_values[..., None])[..., 0], blocked(strength[..., None])[..., 0]))
    heads_out = outputs.transpose(0, 2, 1, 3).reshape(SEQ, HEADS, HEAD)
    head_outputs_mixed = heads_out * lax.rsqrt(lax.optimization_barrier(jnp.mean(heads_out * heads_out, axis=-1, keepdims=True)) + norm_eps)
    head_outputs_mixed = (head_outputs_mixed * head_norm_gain).reshape(SEQ, HEADS * HEAD).astype(jnp.bfloat16)
    group_width = HEADS_DEV * HEAD

    def add_group(running, group_index):
        columns = lax.dynamic_slice_in_dim(head_outputs_mixed, group_index * group_width, group_width, 1)
        weight_rows = lax.dynamic_slice_in_dim(mixer_output_weight, group_index * group_width, group_width, 0)
        partial_value = jnp.dot(columns.astype(jnp.float32), weight_rows.astype(jnp.float32), preferred_element_type=jnp.float32).astype(jnp.bfloat16)
        return (running + lax.optimization_barrier(partial_value).astype(jnp.float32), None)
    mix_total, _ = lax.scan(add_group, jnp.zeros((SEQ, D), jnp.float32), jnp.arange(N_TP, dtype=jnp.int32))
    mix_out = mix_total.astype(jnp.bfloat16)
    exp_normed = rms_scale(expert_input_rows, expert_norm_gain)
    assigned = routes.reshape(-1)
    shares = expert_route_weight.reshape(-1)
    owners = (jnp.arange(EXP_TOKENS * TOP, dtype=jnp.int32) // TOP).astype(jnp.int32)
    most_rows = N_EP * N_TP * CAP

    def expert_pass(running, expert):
        chosen = assigned == expert
        filled = jnp.sum(chosen.astype(jnp.int32))
        picked = jnp.nonzero(chosen, size=most_rows, fill_value=0)[0].astype(jnp.int32)
        live_rows = jnp.arange(most_rows, dtype=jnp.int32) < filled
        token_ids = owners[picked]
        rows_in = exp_normed[token_ids]
        gate_part = jnp.dot(rows_in.astype(jnp.float32), gate_weight[expert].astype(jnp.float32), preferred_element_type=jnp.float32)
        up_part = jnp.dot(rows_in.astype(jnp.float32), up_weight[expert].astype(jnp.float32), preferred_element_type=jnp.float32)
        hidden = (jax.nn.silu(gate_part) * up_part).astype(jnp.bfloat16)
        pieces = jnp.einsum('rgf,gfd->grd', hidden.reshape(most_rows, N_TP, FF_DEV).astype(jnp.float32), down_weight[expert].reshape(N_TP, FF_DEV, D).astype(jnp.float32))
        rounded = lax.optimization_barrier(pieces.astype(jnp.bfloat16)).astype(jnp.float32)
        expert_rows = lax.optimization_barrier(lax.optimization_barrier(jnp.sum(rounded, axis=0)).astype(jnp.bfloat16)).astype(jnp.float32)
        weight_col = jnp.where(live_rows, shares[picked], 0.0)
        return (running.at[token_ids].add(weight_col[:, None] * expert_rows), None)
    exp_total, _ = lax.scan(expert_pass, jnp.zeros((EXP_TOKENS, D), jnp.float32), jnp.arange(EXPERTS, dtype=jnp.int32))
    return (mix_out, exp_total.astype(jnp.bfloat16))
```

```python
import functools

import jax
import jax.numpy as jnp
from jax import lax
from jax.experimental import pallas as pl
from jax.experimental.pallas import tpu as pltpu
from jax.sharding import Mesh
from jax.sharding import PartitionSpec as P

HEAD = 128
BLOCK = 128
EP = ("ep_0", "ep_1")
TP = ("tp_0", "tp_1")
EP_TP = ("ep_0", "ep_1", "tp_0", "tp_1")
F32 = jnp.float32
BF16 = jnp.bfloat16


norm_eps = 1e-06
NN = (((1,), (0,)), ((), ()))
NT = (((1,), (1,)), ((), ()))
TN = (((0,), (0,)), ((), ()))


def mm(a, b, dims=NN):
    return lax.dot_general(a.astype(BF16), b.astype(BF16), dims, preferred_element_type=F32)


def silu(x):
    return x / (1.0 + jnp.exp(-x))


def rms_scale(rows_in, gain_vec):
    widened = rows_in.astype(F32)
    scaled = widened * lax.rsqrt(jnp.mean(widened * widened, axis=-1, keepdims=True) + norm_eps)
    return (scaled * gain_vec).astype(BF16)


def invert_unit_lower(mats, row, col):
    apart = row ^ col
    eye = (row == col).astype(F32)
    size = 1
    invs = None
    while size < BLOCK:
        pick = (apart >= size) & (apart < 2 * size)
        parts = [jnp.where(pick, m, 0.0) for m in mats]
        if invs is None:
            invs = [eye - p for p in parts]
        else:
            invs_low = [x.astype(BF16) for x in invs]
            half = [mm(p, x) for p, x in zip(parts, invs_low)]
            invs = [x - mm(xl, h) for x, xl, h in zip(invs, invs_low, half)]
        size *= 2
    return invs


def terms_kernel(
    count, first_ref, scal_ref, rows_ref, w_ref, extra_ref, corr_ref, shift_ref, qeff_ref, local_ref, last_ref, proj
):
    proj[...] = lax.dot_general(rows_ref[...], w_ref[...], NN, preferred_element_type=F32)
    row = lax.broadcasted_iota(jnp.int32, (BLOCK, BLOCK), 0)
    col = lax.broadcasted_iota(jnp.int32, (BLOCK, BLOCK), 1)
    upper = (row <= col).astype(F32)
    speed, largest = scal_ref[0], scal_ref[1]
    start = first_ref[0] + pl.program_id(0) * count
    mats, keep = [], []
    for b in range(count):
        at = slice(b * BLOCK, (b + 1) * BLOCK)
        q = silu(proj[at, 0:HEAD])
        k = silu(proj[at, HEAD : 2 * HEAD])
        v = silu(proj[at, 2 * HEAD : 3 * HEAD])
        k = k * lax.rsqrt(jnp.sum(k * k, axis=1, keepdims=True) + 1e-06)
        small = proj[at, 3 * HEAD : 4 * HEAD]
        strength = largest * (1.0 / (1.0 + jnp.exp(-small[:, 0:1])))
        flipped = small.T
        x = flipped[0:8, :]
        soft = jnp.maximum(x, 0.0) + jnp.log1p(jnp.exp(-jnp.abs(x)))
        steps = extra_ref[pl.ds(start + b, 1), :] - speed * soft[1:2, :]
        cum_row = lax.dot_general(
            jnp.broadcast_to(steps, (8, BLOCK)), upper, NN, preferred_element_type=F32, precision=lax.Precision.HIGHEST
        )[0:1, :]
        across = jnp.broadcast_to(cum_row, (BLOCK, BLOCK))
        down = across.T
        total = jnp.broadcast_to(cum_row[:, BLOCK - 1 : BLOCK], (BLOCK, BLOCK))
        decay = jnp.exp(jnp.where(row >= col, down - across, -1e30))
        grow = jnp.exp(down)
        both = mm(jnp.concatenate([k, q], axis=0), k, NT)
        mats.append(jnp.where(row > col, both[:BLOCK] * decay * strength, 0.0))
        right = jnp.concatenate([v * strength, k * (grow * strength)], axis=1)
        keep.append((q * grow, both[BLOCK:] * decay, right, k * jnp.exp(total - down)))
        last_ref[b] = jnp.exp(total[0:8, :])
    invs = invert_unit_lower(mats, row, col)
    for b in range(count):
        query_dec, scores, right, keys_dec = keep[b]
        solved = mm(invs[b], right)
        seen = mm(scores, solved)
        kept = mm(keys_dec, solved, TN)
        shift_ref[b] = kept[:, :HEAD]
        corr_ref[b] = kept[:, HEAD:].astype(BF16)
        local_ref[b] = seen[:, :HEAD]
        qeff_ref[b] = (query_dec - seen[:, HEAD:]).astype(BF16)


def block_terms(first, scal, rows, weights, extra, count):
    blocks = rows.shape[0] // BLOCK
    width = weights.shape[1]
    square = lambda kind: jax.ShapeDtypeStruct((blocks, HEAD, HEAD), kind)
    spec = pl.BlockSpec((count, HEAD, HEAD), lambda i: (i, 0, 0))
    return pl.pallas_call(
        functools.partial(terms_kernel, count),
        grid=(blocks // count,),
        out_shape=(square(BF16), square(F32), square(BF16), square(F32), jax.ShapeDtypeStruct((blocks, 8, HEAD), F32)),
        in_specs=[
            pl.BlockSpec(memory_space=pltpu.SMEM),
            pl.BlockSpec(memory_space=pltpu.SMEM),
            pl.BlockSpec((count * BLOCK, rows.shape[1]), lambda i: (i, 0)),
            pl.BlockSpec(weights.shape, lambda i: (0, 0)),
            pl.BlockSpec(extra.shape, lambda i: (0, 0)),
        ],
        out_specs=(spec, spec, spec, spec, pl.BlockSpec((count, 8, HEAD), lambda i: (i, 0, 0))),
        scratch_shapes=[pltpu.VMEM((count * BLOCK, width), F32)],
        compiler_params=pltpu.CompilerParams(vmem_limit_bytes=40 * 1024 * 1024),
        cost_estimate=pl.CostEstimate(
            flops=blocks * 2 * BLOCK * (rows.shape[1] * width + 30 * HEAD * HEAD * 4),
            bytes_accessed=2 * (rows.size + weights.size) + blocks * 12 * HEAD * HEAD,
            transcendentals=0,
        ),
    )(first, scal, rows, weights, extra)


def chain_kernel(corr_ref, shift_ref, qeff_ref, local_ref, last_ref, g_ref, h_ref, ab_ref):
    blocks = corr_ref.shape[0]
    row = lax.broadcasted_iota(jnp.int32, (HEAD, HEAD), 0)
    col = lax.broadcasted_iota(jnp.int32, (HEAD, HEAD), 1)
    maps = (row == col).astype(F32)
    memory = jnp.zeros((HEAD, HEAD), F32)
    for j in range(blocks):
        both = jnp.concatenate([maps, memory], axis=1).astype(BF16)
        out = mm(qeff_ref[j], both)
        g_ref[j * BLOCK : (j + 1) * BLOCK, :] = out[:, :HEAD].astype(BF16)
        h_ref[j * BLOCK : (j + 1) * BLOCK, :] = out[:, HEAD:] + local_ref[j]
        moved = mm(corr_ref[j], both)
        last = last_ref[j, 0:1, :]
        maps = maps * last - moved[:, :HEAD]
        memory = memory * last - moved[:, HEAD:] + shift_ref[j]
    ab_ref[:, :HEAD] = maps.astype(BF16)
    ab_ref[:, HEAD:] = memory.astype(BF16)


def chain_blocks(corr, shift, qeff, local, last):
    rows = corr.shape[0] * BLOCK
    return pl.pallas_call(
        chain_kernel,
        out_shape=(
            jax.ShapeDtypeStruct((rows, HEAD), BF16),
            jax.ShapeDtypeStruct((rows, HEAD), F32),
            jax.ShapeDtypeStruct((HEAD, 2 * HEAD), BF16),
        ),
        cost_estimate=pl.CostEstimate(flops=rows * 8 * HEAD * HEAD, bytes_accessed=rows * HEAD * 20, transcendentals=0),
    )(corr, shift, qeff, local, last)


def row_kernel(here_ref, own_ref, one_ref, two_ref, three_ref, before_ref, total_ref, slots):
    here = here_ref[0]
    slots[here] = own_ref[...]
    slots[(here + 3) % 4] = one_ref[...]
    slots[(here + 2) % 4] = two_ref[...]
    slots[(here + 1) % 4] = three_ref[...]
    row = lax.broadcasted_iota(jnp.int32, (HEAD, 2 * HEAD), 0)
    col = lax.broadcasted_iota(jnp.int32, (HEAD, 2 * HEAD), 1)
    eye = (row == col).astype(F32)
    so_far = slots[0].astype(F32)
    before = jnp.where(here == 0, eye, so_far)
    for k in range(1, 4):
        piece = slots[k]
        own = jnp.where(col >= HEAD, piece.astype(F32), 0.0)
        so_far = mm(piece[:, :HEAD], so_far) + own
        if k < 3:
            before = jnp.where(here > k, so_far, before)
    before_ref[...] = before
    total_ref[...] = so_far.astype(BF16)


def compose_row(here, own, one, two, three):
    vmem = pl.BlockSpec(memory_space=pltpu.VMEM)
    return pl.pallas_call(
        row_kernel,
        out_shape=(jax.ShapeDtypeStruct((HEAD, 2 * HEAD), F32), jax.ShapeDtypeStruct((HEAD, 2 * HEAD), BF16)),
        in_specs=[pl.BlockSpec(memory_space=pltpu.SMEM)] + [vmem] * 4,
        out_specs=(vmem, vmem),
        scratch_shapes=[pltpu.VMEM((4, HEAD, 2 * HEAD), BF16)],
        cost_estimate=pl.CostEstimate(flops=12 * HEAD**3, bytes_accessed=8 * HEAD * HEAD, transcendentals=0),
    )(here, own, one, two, three)


def apply_kernel(here_ref, one_ref, two_ref, three_ref, before_ref, g_ref, h_ref, gain_ref, out_ref, slots):
    here = here_ref[0]
    slots[(here + 3) % 4] = one_ref[...]
    slots[(here + 2) % 4] = two_ref[...]
    slots[(here + 1) % 4] = three_ref[...]
    memory = jnp.where(here > 0, slots[0][:, HEAD:].astype(F32), 0.0)
    for k in range(1, 3):
        piece = slots[k]
        moved = mm(piece[:, :HEAD], memory) + piece[:, HEAD:].astype(F32)
        memory = jnp.where(here > k, moved, memory)
    memory = mm(before_ref[:, :HEAD], memory) + before_ref[:, HEAD:]
    heads_out = mm(g_ref[...], memory) + h_ref[...]
    scale = lax.rsqrt(jnp.mean(heads_out * heads_out, axis=1, keepdims=True) + norm_eps)
    out_ref[...] = (heads_out * scale * gain_ref[...]).astype(BF16)


def apply_memory(here, one, two, three, before, g, h, gain):
    vmem = pl.BlockSpec(memory_space=pltpu.VMEM)
    return pl.pallas_call(
        apply_kernel,
        out_shape=jax.ShapeDtypeStruct(h.shape, BF16),
        in_specs=[pl.BlockSpec(memory_space=pltpu.SMEM)] + [vmem] * 7,
        out_specs=vmem,
        scratch_shapes=[pltpu.VMEM((4, HEAD, 2 * HEAD), BF16)],
        cost_estimate=pl.CostEstimate(flops=h.size * 2 * HEAD, bytes_accessed=h.size * 8, transcendentals=0),
    )(here, one, two, three, before, g, h, gain.reshape(1, HEAD))


def around(x, axis):
    size = lax.axis_size(axis)
    return [lax.ppermute(x, axis, [(i, (i + k) % size) for i in range(size)]) for k in range(1, size)]


def slot_numbers(routes, experts, capacity):
    assigned = routes.reshape(-1)
    onehot = (assigned[:, None] == jnp.arange(experts, dtype=jnp.int32)[None, :]).astype(jnp.int32)
    before = jnp.cumsum(onehot, axis=0) - onehot
    return assigned * capacity + jnp.sum(before * onehot, axis=1)


def body(
    mixer_input_rows,
    mixer_norm_gain,
    query_weight,
    key_weight,
    value_weight,
    write_strength_projection,
    decay_projection,
    head_decay_speed,
    largest_write_strength,
    extra_log_decay,
    head_norm_gain,
    mixer_output_weight,
    expert_input_rows,
    expert_norm_gain,
    routes,
    expert_route_weight,
    gate_weight,
    up_weight,
    down_weight,
):
    head = lax.axis_index(TP)
    core = lax.axis_index("tp_1")
    ring_size = lax.axis_size("tp_0")
    model_width = mixer_input_rows.shape[1]

    mix_normed = rms_scale(mixer_input_rows, mixer_norm_gain)
    mix_rows = lax.all_gather(mix_normed, TP, axis=0, tiled=True)

    exp_normed = rms_scale(expert_input_rows, expert_norm_gain)
    token_count, top_count = routes.shape
    experts = gate_weight.shape[0] * lax.axis_size(EP)
    capacity = (3 * top_count * token_count + 2 * experts - 1) // (2 * experts)
    slot_ids = slot_numbers(routes, experts, capacity)
    places = jnp.arange(experts * capacity, dtype=jnp.int32)
    chosen = slot_ids.reshape(token_count, top_count)[None, :, :] == places[:, None, None]
    selector = jnp.sum(chosen.astype(F32), axis=2)
    sending = jnp.dot(selector.astype(BF16), exp_normed, preferred_element_type=F32).astype(BF16)
    arrived = lax.all_to_all(
        sending.reshape(experts, capacity, model_width), EP, split_axis=0, concat_axis=0, tiled=True
    ).reshape(-1, model_width)
    exp_rows = lax.all_gather(arrived, TP, axis=0, tiled=True)

    weights = jnp.concatenate(
        [
            query_weight,
            key_weight,
            value_weight,
            lax.dynamic_slice_in_dim(write_strength_projection, head, 1, 1),
            lax.dynamic_slice_in_dim(decay_projection, head, 1, 1),
            jnp.zeros((model_width, HEAD - 2), BF16),
        ],
        axis=1,
    )
    scal = jnp.concatenate([head_decay_speed, largest_write_strength])
    extra = extra_log_decay.reshape(-1, BLOCK)
    terms = block_terms(jnp.zeros((1,), jnp.int32), scal, mix_rows, weights, extra, 8)
    gains, local, span = chain_blocks(*terms)
    before, total = compose_row(lax.axis_index("ep_1")[None], span, *around(span, "ep_1"))
    mixed = apply_memory(
        lax.axis_index("ep_0")[None], *around(total, "ep_0"), before, gains, local, head_norm_gain
    )

    by_head = lax.all_to_all(mixed.reshape(-1, BLOCK, HEAD), TP, split_axis=0, concat_axis=0, tiled=True)
    w_whole = lax.all_gather(mixer_output_weight, TP, axis=0, tiled=True)
    mix_out = lax.dot_general(
        by_head.transpose(1, 0, 2).reshape(BLOCK, -1), w_whole, NN, preferred_element_type=F32
    ).astype(BF16)

    gate_part = jnp.dot(exp_rows, gate_weight[0], preferred_element_type=F32)
    up_part = jnp.dot(exp_rows, up_weight[0], preferred_element_type=F32)
    hidden = (jax.nn.silu(gate_part) * up_part).astype(BF16)
    hidden = hidden.reshape(ring_size, 2, -1, hidden.shape[1])
    share = hidden.shape[2]

    def down_for(owner):
        rows = lax.dynamic_slice_in_dim(hidden, owner, 1, 1).reshape(ring_size * share, -1)
        return jnp.dot(rows, down_weight[0], preferred_element_type=F32)

    theirs = lax.ppermute(down_for(1 - core).astype(BF16), "tp_1", [(0, 1), (1, 0)])
    pair = (down_for(core) + theirs.astype(F32)).astype(BF16).reshape(ring_size, share, model_width)
    pieces = lax.all_to_all(pair, "tp_0", split_axis=0, concat_axis=0, tiled=True)
    finished = jnp.sum(pieces.astype(F32), axis=0).astype(BF16)
    returned = lax.all_to_all(
        finished.reshape(experts, capacity, model_width), EP, split_axis=0, concat_axis=0, tiled=True
    ).reshape(experts * capacity, model_width)
    scaled = jnp.sum(chosen.astype(F32) * expert_route_weight[None, :, :], axis=2)
    exp_out = lax.dot_general(
        scaled, returned.astype(F32), TN, preferred_element_type=F32, precision=lax.Precision.HIGHEST
    ).astype(BF16)
    return (mix_out, exp_out)


def solution(mesh):
    torus = Mesh(mesh.devices.reshape(4, 4, 8, 2), ("ep_0", "ep_1", "tp_0", "tp_1"))
    placed = (
        P(EP_TP, None),
        P(),
        P(None, TP),
        P(None, TP),
        P(None, TP),
        P(),
        P(),
        P(TP),
        P(TP),
        P(EP, TP),
        P(),
        P(TP, None),
        P(EP_TP, None),
        P(),
        P(EP_TP, None),
        P(EP_TP, None),
        P(EP, None, TP),
        P(EP, None, TP),
        P(EP, TP, None),
    )
    return jax.shard_map(
        body,
        mesh=torus,
        in_specs=placed,
        out_specs=(P(EP_TP, None), P(EP_TP, None)),
        check_vma=False,
    )
```

```python
import functools

import jax
import jax.numpy as jnp
from jax import lax
from jax.experimental import pallas as pl
from jax.experimental.pallas import tpu as pltpu
from jax.sharding import Mesh
from jax.sharding import PartitionSpec as P


HEAD = 128
BLOCK = 128
EP = ("ep_0", "ep_1")
TP = ("tp_0", "tp_1")
EP_TP = ("ep_0", "ep_1", "tp_0", "tp_1")
F32 = jnp.float32
BF16 = jnp.bfloat16


norm_eps = 1e-06
NN = (((1,), (0,)), ((), ()))
NT = (((1,), (1,)), ((), ()))
TN = (((0,), (0,)), ((), ()))


def mm(a, b, dims=NN):
    return lax.dot_general(a.astype(BF16), b.astype(BF16), dims, preferred_element_type=F32)


def silu(x):
    return x / (1.0 + jnp.exp(-x))


def rms_scale(rows_in, gain_vec):
    widened = rows_in.astype(F32)
    scaled = widened * lax.rsqrt(jnp.mean(widened * widened, axis=-1, keepdims=True) + norm_eps)
    return (scaled * gain_vec).astype(BF16)


def invert_unit_lower(mats, row, col):
    apart = row ^ col
    eye = (row == col).astype(F32)
    size = 1
    invs = None
    while size < BLOCK:
        pick = (apart >= size) & (apart < 2 * size)
        parts = [jnp.where(pick, m, 0.0) for m in mats]
        if invs is None:
            invs = [eye - p for p in parts]
        else:
            invs_low = [x.astype(BF16) for x in invs]
            half = [mm(p, x) for p, x in zip(parts, invs_low)]
            invs = [x - mm(xl, h) for x, xl, h in zip(invs, invs_low, half)]
        size *= 2
    return invs


def weights_kernel(head_ref, q_ref, k_ref, v_ref, strength_ref, decay_ref, out_ref):
    out_ref[:, 0:HEAD] = q_ref[...]
    out_ref[:, HEAD : 2 * HEAD] = k_ref[...]
    out_ref[:, 2 * HEAD : 3 * HEAD] = v_ref[...]
    heads = strength_ref.shape[1]
    row = lax.broadcasted_iota(jnp.int32, (heads, HEAD), 0)
    col = lax.broadcasted_iota(jnp.int32, (heads, HEAD), 1)
    here = row == head_ref[0]
    first = (here & (col == 0)).astype(BF16)
    second = (here & (col == 1)).astype(BF16)
    out_ref[:, 3 * HEAD :] = (mm(strength_ref[...], first) + mm(decay_ref[...], second)).astype(BF16)


def join_weights(head, query, key, value, strength, decay):
    depth = query.shape[0]
    step = depth // 4
    tall = lambda x: pl.BlockSpec((step, x.shape[1]), lambda i: (i, 0))
    return pl.pallas_call(
        weights_kernel,
        grid=(4,),
        out_shape=jax.ShapeDtypeStruct((depth, 4 * HEAD), BF16),
        in_specs=[pl.BlockSpec(memory_space=pltpu.SMEM)] + [tall(x) for x in (query, key, value, strength, decay)],
        out_specs=pl.BlockSpec((step, 4 * HEAD), lambda i: (i, 0)),
        cost_estimate=pl.CostEstimate(flops=10**8, bytes_accessed=depth * HEAD * 16, transcendentals=0),
    )(head, query, key, value, strength, decay)


def terms_kernel(pieces, ids_ref, scal_ref, *refs):
    rows_refs = refs[:pieces]
    w_ref, extra_ref, low_ref, high_ref, last_ref, proj = refs[pieces:]
    rows = jnp.concatenate([r[...] for r in rows_refs], axis=0)
    count = rows.shape[0] // BLOCK
    proj[...] = lax.dot_general(rows, w_ref[...], NN, preferred_element_type=F32)
    row = lax.broadcasted_iota(jnp.int32, (BLOCK, BLOCK), 0)
    col = lax.broadcasted_iota(jnp.int32, (BLOCK, BLOCK), 1)
    upper = (row <= col).astype(F32)
    speed, largest = scal_ref[0], scal_ref[1]
    mats, keep = [], []
    for b in range(count):
        at = slice(b * BLOCK, (b + 1) * BLOCK)
        q = silu(proj[at, 0:HEAD])
        k = silu(proj[at, HEAD : 2 * HEAD])
        v = silu(proj[at, 2 * HEAD : 3 * HEAD])
        k = k * lax.rsqrt(jnp.sum(k * k, axis=1, keepdims=True) + 1e-06)
        small = proj[at, 3 * HEAD : 4 * HEAD]
        strength = largest * (1.0 / (1.0 + jnp.exp(-small[:, 0:1])))
        flipped = small.T
        x = flipped[0:8, :]
        soft = jnp.maximum(x, 0.0) + jnp.log1p(jnp.exp(-jnp.abs(x)))
        steps = extra_ref[pl.ds(ids_ref[b], 1), :] - speed * soft[1:2, :]
        cum_row = lax.dot_general(
            jnp.broadcast_to(steps, (8, BLOCK)), upper, NN, preferred_element_type=F32, precision=lax.Precision.HIGHEST
        )[0:1, :]
        across = jnp.broadcast_to(cum_row, (BLOCK, BLOCK))
        down = across.T
        total = jnp.broadcast_to(cum_row[:, BLOCK - 1 : BLOCK], (BLOCK, BLOCK))
        decay = jnp.exp(jnp.where(row >= col, down - across, -1e30))
        grow = jnp.exp(down)
        both = mm(jnp.concatenate([k, q], axis=0), k, NT)
        mats.append(jnp.where(row > col, both[:BLOCK] * decay * strength, 0.0))
        right = jnp.concatenate([v * strength, k * (grow * strength)], axis=1)
        keep.append((q * grow, both[BLOCK:] * decay, right, k * jnp.exp(total - down)))
        last_ref[b] = jnp.exp(total[0:8, :])
    invs = invert_unit_lower(mats, row, col)
    for b in range(count):
        query_dec, scores, right, keys_dec = keep[b]
        solved = mm(invs[b], right)
        seen = mm(scores, solved)
        kept = mm(keys_dec, solved, TN)
        high_ref[b, :, :HEAD] = kept[:, :HEAD]
        high_ref[b, :, HEAD:] = seen[:, :HEAD]
        low_ref[b, :HEAD, :] = (query_dec - seen[:, HEAD:]).astype(BF16)
        low_ref[b, HEAD:, :] = kept[:, HEAD:].astype(BF16)


def block_terms(ids, scal, rows, weights, extra):
    total = sum(r.shape[0] for r in rows)
    blocks = total // BLOCK
    width = weights.shape[1]
    smem = pl.BlockSpec(memory_space=pltpu.SMEM)
    vmem = pl.BlockSpec(memory_space=pltpu.VMEM)
    return pl.pallas_call(
        functools.partial(terms_kernel, len(rows)),
        out_shape=(
            jax.ShapeDtypeStruct((blocks, 2 * HEAD, HEAD), BF16),
            jax.ShapeDtypeStruct((blocks, HEAD, 2 * HEAD), F32),
            jax.ShapeDtypeStruct((blocks, 8, HEAD), F32),
        ),
        in_specs=[smem, smem] + [vmem] * (len(rows) + 2),
        out_specs=(vmem, vmem, vmem),
        scratch_shapes=[pltpu.VMEM((total, width), F32)],
        cost_estimate=pl.CostEstimate(
            flops=blocks * 2 * BLOCK * (rows[0].shape[1] * width + 30 * HEAD * HEAD * 4),
            bytes_accessed=2 * (total * rows[0].shape[1] + weights.size) + blocks * 12 * HEAD * HEAD,
            transcendentals=0,
        ),
    )(ids, scal, *rows, weights, extra)


def chain_kernel(sizes, ids_ref, *refs):
    sets = len(sizes)
    lows, highs, lasts = refs[:sets], refs[sets : 2 * sets], refs[2 * sets : 3 * sets]
    g_ref, h_ref, ab_ref, low_scr, high_scr, last_scr = refs[3 * sets :]
    at = 0
    for s, size in enumerate(sizes):
        for b in range(size):
            slot = ids_ref[at]
            low_scr[slot] = lows[s][b]
            high_scr[slot] = highs[s][b]
            last_scr[slot] = lasts[s][b]
            at += 1
    row = lax.broadcasted_iota(jnp.int32, (HEAD, HEAD), 0)
    col = lax.broadcasted_iota(jnp.int32, (HEAD, HEAD), 1)
    maps = (row == col).astype(F32)
    memory = jnp.zeros((HEAD, HEAD), F32)
    for j in range(at):
        both = jnp.concatenate([maps, memory], axis=1).astype(BF16)
        out = mm(low_scr[j], both)
        g_ref[j * BLOCK : (j + 1) * BLOCK, :] = out[:HEAD, :HEAD].astype(BF16)
        h_ref[j * BLOCK : (j + 1) * BLOCK, :] = out[:HEAD, HEAD:] + high_scr[j, :, HEAD:]
        last = last_scr[j, 0:1, :]
        maps = maps * last - out[HEAD:, :HEAD]
        memory = memory * last - out[HEAD:, HEAD:] + high_scr[j, :, :HEAD]
    ab_ref[:, :HEAD] = maps.astype(BF16)
    ab_ref[:, HEAD:] = memory.astype(BF16)


def chain_blocks(ids, lows, highs, lasts):
    sizes = tuple(x.shape[0] for x in lows)
    blocks = sum(sizes)
    rows = blocks * BLOCK
    vmem = pl.BlockSpec(memory_space=pltpu.VMEM)
    return pl.pallas_call(
        functools.partial(chain_kernel, sizes),
        out_shape=(
            jax.ShapeDtypeStruct((rows, HEAD), BF16),
            jax.ShapeDtypeStruct((rows, HEAD), F32),
            jax.ShapeDtypeStruct((HEAD, 2 * HEAD), BF16),
        ),
        in_specs=[pl.BlockSpec(memory_space=pltpu.SMEM)] + [vmem] * (3 * len(sizes)),
        out_specs=(vmem, vmem, vmem),
        scratch_shapes=[
            pltpu.VMEM((blocks, 2 * HEAD, HEAD), BF16),
            pltpu.VMEM((blocks, HEAD, 2 * HEAD), F32),
            pltpu.VMEM((blocks, 8, HEAD), F32),
        ],
        cost_estimate=pl.CostEstimate(flops=rows * 8 * HEAD * HEAD, bytes_accessed=rows * HEAD * 20, transcendentals=0),
    )(ids, *lows, *highs, *lasts)


def row_kernel(here_ref, own_ref, one_ref, two_ref, three_ref, before_ref, total_ref, slots):
    here = here_ref[0]
    slots[here] = own_ref[...]
    slots[(here + 3) % 4] = one_ref[...]
    slots[(here + 2) % 4] = two_ref[...]
    slots[(here + 1) % 4] = three_ref[...]
    row = lax.broadcasted_iota(jnp.int32, (HEAD, 2 * HEAD), 0)
    col = lax.broadcasted_iota(jnp.int32, (HEAD, 2 * HEAD), 1)
    eye = (row == col).astype(F32)
    so_far = slots[0].astype(F32)
    before = jnp.where(here == 0, eye, so_far)
    for k in range(1, 4):
        piece = slots[k]
        own = jnp.where(col >= HEAD, piece.astype(F32), 0.0)
        so_far = mm(piece[:, :HEAD], so_far) + own
        if k < 3:
            before = jnp.where(here > k, so_far, before)
    before_ref[...] = before
    total_ref[...] = so_far.astype(BF16)


def compose_row(here, own, one, two, three):
    vmem = pl.BlockSpec(memory_space=pltpu.VMEM)
    return pl.pallas_call(
        row_kernel,
        out_shape=(jax.ShapeDtypeStruct((HEAD, 2 * HEAD), F32), jax.ShapeDtypeStruct((HEAD, 2 * HEAD), BF16)),
        in_specs=[pl.BlockSpec(memory_space=pltpu.SMEM)] + [vmem] * 4,
        out_specs=(vmem, vmem),
        scratch_shapes=[pltpu.VMEM((4, HEAD, 2 * HEAD), BF16)],
        compiler_params=pltpu.CompilerParams(vmem_limit_bytes=8 * 1024 * 1024),
        cost_estimate=pl.CostEstimate(flops=12 * HEAD**3, bytes_accessed=8 * HEAD * HEAD, transcendentals=0),
    )(here, own, one, two, three)


def apply_kernel(here_ref, one_ref, two_ref, three_ref, before_ref, g_ref, h_ref, gain_ref, out_ref, slots):
    here = here_ref[0]
    slots[(here + 3) % 4] = one_ref[...]
    slots[(here + 2) % 4] = two_ref[...]
    slots[(here + 1) % 4] = three_ref[...]
    memory = jnp.where(here > 0, slots[0][:, HEAD:].astype(F32), 0.0)
    for k in range(1, 3):
        piece = slots[k]
        moved = mm(piece[:, :HEAD], memory) + piece[:, HEAD:].astype(F32)
        memory = jnp.where(here > k, moved, memory)
    memory = mm(before_ref[:, :HEAD], memory) + before_ref[:, HEAD:]
    heads_out = mm(g_ref[...], memory) + h_ref[...]
    scale = lax.rsqrt(jnp.mean(heads_out * heads_out, axis=1, keepdims=True) + norm_eps)
    out_ref[...] = (heads_out * scale * gain_ref[...]).astype(BF16)


def apply_memory(here, one, two, three, before, g, h, gain):
    vmem = pl.BlockSpec(memory_space=pltpu.VMEM)
    return pl.pallas_call(
        apply_kernel,
        out_shape=jax.ShapeDtypeStruct(h.shape, BF16),
        in_specs=[pl.BlockSpec(memory_space=pltpu.SMEM)] + [vmem] * 7,
        out_specs=vmem,
        scratch_shapes=[pltpu.VMEM((4, HEAD, 2 * HEAD), BF16)],
        compiler_params=pltpu.CompilerParams(vmem_limit_bytes=8 * 1024 * 1024),
        cost_estimate=pl.CostEstimate(flops=h.size * 2 * HEAD, bytes_accessed=h.size * 8, transcendentals=0),
    )(here, one, two, three, before, g, h, gain.reshape(1, HEAD))


def output_kernel(core_ref, x_ref, w_ref, mine_ref, theirs_ref, total):
    step = pl.program_id(0)

    @pl.when(step == 0)
    def _():
        total[...] = jnp.zeros_like(total)

    rows = jnp.concatenate([x_ref[0], x_ref[1]], axis=1)
    total[...] += mm(rows, w_ref[...])

    @pl.when(step == pl.num_programs(0) - 1)
    def _():
        first = core_ref[0] == 0
        mine_ref[...] = jnp.where(first, total[:BLOCK], total[BLOCK:])
        theirs_ref[...] = jnp.where(first, total[BLOCK:], total[:BLOCK]).astype(BF16)


def output_product(core, by_head, weights):
    depth, width = weights.shape
    whole = lambda i: (0, 0)
    return pl.pallas_call(
        output_kernel,
        grid=(depth // (2 * HEAD),),
        out_shape=(jax.ShapeDtypeStruct((BLOCK, width), F32), jax.ShapeDtypeStruct((BLOCK, width), BF16)),
        in_specs=[
            pl.BlockSpec(memory_space=pltpu.SMEM),
            pl.BlockSpec((2, 2 * BLOCK, HEAD), lambda i: (i, 0, 0)),
            pl.BlockSpec((2 * HEAD, width), lambda i: (i, 0)),
        ],
        out_specs=(pl.BlockSpec((BLOCK, width), whole), pl.BlockSpec((BLOCK, width), whole)),
        scratch_shapes=[pltpu.VMEM((2 * BLOCK, width), F32)],
        cost_estimate=pl.CostEstimate(
            flops=4 * BLOCK * depth * width, bytes_accessed=2 * depth * width, transcendentals=0
        ),
    )(core, by_head.reshape(-1, 2 * BLOCK, HEAD), weights)


def expert_kernel(core_ref, rows_ref, gate_ref, up_ref, down_ref, mine_ref, theirs_ref, rows, gate, up, down, sems):
    core = core_ref[0]
    copies = [
        pltpu.make_async_copy(rows_ref.at[:, core], rows.at[0], sems.at[0]),
        pltpu.make_async_copy(rows_ref.at[:, 1 - core], rows.at[1], sems.at[1]),
        pltpu.make_async_copy(gate_ref, gate, sems.at[2]),
        pltpu.make_async_copy(up_ref, up, sems.at[3]),
        pltpu.make_async_copy(down_ref, down, sems.at[4]),
    ]
    for copy in copies:
        copy.start()
    for copy in copies[:3]:
        copy.wait()
    x = rows[...].reshape(-1, rows.shape[-1])
    half = x.shape[0] // 2
    gated = silu(mm(x, gate[...], NT))
    copies[3].wait()
    hidden = (gated * mm(x, up[...], NT)).astype(BF16)
    copies[4].wait()
    theirs_ref[...] = mm(hidden[half:], down[...]).astype(BF16)
    mine_ref[...] = mm(hidden[:half], down[...]).astype(BF16)


def expert_sums(core, rows, gate, up, down):
    ring, _, share, width = rows.shape
    units = gate.shape[0]
    vmem = pl.BlockSpec(memory_space=pltpu.VMEM)
    out = jax.ShapeDtypeStruct((ring * share, width), BF16)
    return pl.pallas_call(
        expert_kernel,
        out_shape=(out, out),
        in_specs=[pl.BlockSpec(memory_space=pltpu.SMEM)] + [pl.BlockSpec(memory_space=pl.ANY)] * 4,
        out_specs=(vmem, vmem),
        scratch_shapes=[
            pltpu.VMEM((2, ring, share, width), BF16),
            pltpu.VMEM((units, width), BF16),
            pltpu.VMEM((units, width), BF16),
            pltpu.VMEM((units, width), BF16),
            pltpu.SemaphoreType.DMA((5,)),
        ],
        cost_estimate=pl.CostEstimate(
            flops=12 * ring * share * width * units, bytes_accessed=6 * units * width + 8 * ring * share * width,
            transcendentals=0,
        ),
    )(core, rows, gate, up, down)


def around(x, axis):
    size = lax.axis_size(axis)
    out = []
    for k in range(1, size):
        out.append(lax.ppermute(x, axis, [(i, (i + k) % size) for i in range(size)]))
    return out


def slot_numbers(routes, experts, capacity):
    assigned = routes.reshape(-1)
    onehot = (assigned[:, None] == jnp.arange(experts, dtype=jnp.int32)[None, :]).astype(jnp.int32)
    before = jnp.cumsum(onehot, axis=0) - onehot
    return assigned * capacity + jnp.sum(before * onehot, axis=1)


def mixed_step(
    mixer_input_rows,
    mixer_norm_gain,
    query_weight,
    key_weight,
    value_weight,
    write_strength_projection,
    decay_projection,
    head_decay_speed,
    largest_write_strength,
    extra_log_decay,
    head_norm_gain,
    mixer_output_weight,
    expert_input_rows,
    expert_norm_gain,
    routes,
    expert_route_weight,
    gate_weight,
    up_weight,
    down_weight,
):
    head = lax.axis_index(TP)
    core = lax.axis_index("tp_1")
    ring_size = lax.axis_size("tp_0")
    model_width = mixer_input_rows.shape[1]

    mix_normed = rms_scale(mixer_input_rows, mixer_norm_gain)
    here = lax.axis_index("tp_0")
    other = 1 - core
    right = [(i, (i + 1) % ring_size) for i in range(ring_size)]
    left = [(i, (i - 1) % ring_size) for i in range(ring_size)]
    swap = [(0, 1), (1, 0)]
    cross = lambda x: lax.ppermute(x, "tp_1", swap)
    half = ring_size // 2
    split = BLOCK // 2

    exp_normed = rms_scale(expert_input_rows, expert_norm_gain)
    token_count, top_count = routes.shape
    experts = gate_weight.shape[0] * lax.axis_size(EP)
    capacity = (3 * top_count * token_count + 2 * experts - 1) // (2 * experts)
    slot_ids = slot_numbers(routes, experts, capacity)
    places = jnp.arange(experts * capacity, dtype=jnp.int32)
    chosen = slot_ids.reshape(token_count, top_count)[None, :, :] == places[:, None, None]
    selector = jnp.sum(chosen.astype(F32), axis=2)
    sending = jnp.dot(selector.astype(BF16), exp_normed, preferred_element_type=F32).astype(BF16)
    arrived = lax.all_to_all(
        sending.reshape(experts, capacity, model_width), EP, split_axis=0, concat_axis=0, tiled=True
    ).reshape(-1, model_width)
    exp_rows = lax.all_gather(arrived, TP, axis=0, tiled=True)

    weights = join_weights(
        head[None], query_weight, key_weight, value_weight, write_strength_projection, decay_projection
    )
    scal = jnp.concatenate([head_decay_speed, largest_write_strength])
    extra = extra_log_decay.reshape(-1, BLOCK)
    groups = [([mix_normed, cross(mix_normed)], [2 * here + core, 2 * here + other])]
    from_left, from_right = mix_normed, mix_normed
    for k in range(1, half):
        from_left = lax.ppermute(from_left, "tp_0", right)
        from_right = lax.ppermute(from_right, "tp_0", left)
        low, high = (here - k) % ring_size, (here + k) % ring_size
        groups.append(
            (
                [from_left, from_right, cross(from_left), cross(from_right)],
                [2 * low + core, 2 * high + core, 2 * low + other, 2 * high + other],
            )
        )
    top = lax.ppermute(from_left[:split], "tp_0", right)
    bottom = lax.ppermute(from_right[split:], "tp_0", left)
    far = (here + half) % ring_size
    groups.append(([top, bottom, cross(top), cross(bottom)], [2 * far + core, 2 * far + other]))
    places_of = [jnp.stack(ids).astype(jnp.int32) for _, ids in groups]
    terms = []
    for ids, (rows, _) in zip(places_of, groups):
        terms.append(block_terms(ids, scal, rows, weights, extra))
    gains, local, span = chain_blocks(jnp.concatenate(places_of), *[[t[i] for t in terms] for i in range(3)])
    before, total = compose_row(lax.axis_index("ep_1")[None], span, *around(span, "ep_1"))
    mixed = apply_memory(lax.axis_index("ep_0")[None], *around(total, "ep_0"), before, gains, local, head_norm_gain)

    by_head = lax.all_to_all(mixed, "tp_0", split_axis=0, concat_axis=0, tiled=True)
    w_own = lax.all_gather(mixer_output_weight, "tp_0", axis=0, tiled=True)
    mix_mine, mix_theirs = output_product(core[None], by_head, w_own)
    mix_out = (mix_mine + cross(mix_theirs).astype(F32)).astype(BF16)

    share = experts * capacity
    mine, theirs = expert_sums(
        core[None],
        exp_rows.reshape(ring_size, 2, share, model_width),
        gate_weight[0].T,
        up_weight[0].T,
        down_weight[0],
    )
    crossed = cross(theirs)
    pair = (mine.astype(F32) + crossed.astype(F32)).astype(BF16).reshape(ring_size, share, model_width)
    pieces = lax.all_to_all(pair, "tp_0", split_axis=0, concat_axis=0, tiled=True)
    finished = jnp.sum(pieces.astype(F32), axis=0).astype(BF16)
    returned = lax.all_to_all(
        finished.reshape(experts, capacity, model_width), EP, split_axis=0, concat_axis=0, tiled=True
    ).reshape(experts * capacity, model_width)
    scaled = jnp.sum(chosen.astype(F32) * expert_route_weight[None, :, :], axis=2)
    exp_out = lax.dot_general(
        scaled, returned.astype(F32), TN, preferred_element_type=F32, precision=lax.Precision.HIGHEST
    ).astype(BF16)
    return (mix_out, exp_out)


def solution(mesh):
    torus = Mesh(mesh.devices.reshape(4, 4, 8, 2), ("ep_0", "ep_1", "tp_0", "tp_1"))
    placed = (
        P(EP_TP, None),
        P(),
        P(None, TP),
        P(None, TP),
        P(None, TP),
        P(),
        P(),
        P(TP),
        P(TP),
        P(EP, TP),
        P(),
        P(TP, None),
        P(EP_TP, None),
        P(),
        P(EP_TP, None),
        P(EP_TP, None),
        P(EP, None, TP),
        P(EP, None, TP),
        P(EP, TP, None),
    )
    return jax.shard_map(
        mixed_step,
        mesh=torus,
        in_specs=placed,
        out_specs=(P(EP_TP, None), P(EP_TP, None)),
        check_vma=False,
    )
```

```python
import functools

import jax
import jax.numpy as jnp
from jax import lax
from jax.experimental import pallas as pl
from jax.experimental.pallas import tpu as pltpu
from jax.sharding import Mesh
from jax.sharding import PartitionSpec as P


HEAD = 128
BLOCK = 128
TOKENS = 8
SLOTS = 2
EP = ("ep_0", "ep_1")
TP = ("tp_0", "tp_1")
EP_TP = ("ep_0", "ep_1", "tp_0", "tp_1")
F32 = jnp.float32
BF16 = jnp.bfloat16


norm_eps = 1e-06
NN = (((1,), (0,)), ((), ()))
NT = (((1,), (1,)), ((), ()))
TN = (((0,), (0,)), ((), ()))


def mm(a, b, dims=NN):
    return lax.dot_general(a.astype(BF16), b.astype(BF16), dims, preferred_element_type=F32)


def silu(x):
    return x / (1.0 + jnp.exp(-x))


def rms_scale(rows_in, gain_vec):
    widened = rows_in.astype(F32)
    scaled = widened * lax.rsqrt(jnp.mean(widened * widened, axis=-1, keepdims=True) + norm_eps)
    return (scaled * gain_vec).astype(BF16)


def invert_unit_lower(mats, row, col):
    apart = row ^ col
    eye = (row == col).astype(F32)
    size = 1
    invs = None
    while size < BLOCK:
        pick = (apart >= size) & (apart < 2 * size)
        parts = [jnp.where(pick, m, 0.0) for m in mats]
        if invs is None:
            invs = [eye - p for p in parts]
        else:
            invs_low = [x.astype(BF16) for x in invs]
            half = [mm(p, x) for p, x in zip(parts, invs_low)]
            invs = [x - mm(xl, h) for x, xl, h in zip(invs, invs_low, half)]
        size *= 2
    return invs


def weights_kernel(head_ref, q_ref, k_ref, v_ref, strength_ref, decay_ref, out_ref):
    out_ref[:, 0:HEAD] = q_ref[...]
    out_ref[:, HEAD : 2 * HEAD] = k_ref[...]
    out_ref[:, 2 * HEAD : 3 * HEAD] = v_ref[...]
    heads = strength_ref.shape[1]
    row = lax.broadcasted_iota(jnp.int32, (heads, HEAD), 0)
    col = lax.broadcasted_iota(jnp.int32, (heads, HEAD), 1)
    here = row == head_ref[0]
    first = (here & (col == 0)).astype(BF16)
    second = (here & (col == 1)).astype(BF16)
    out_ref[:, 3 * HEAD :] = (mm(strength_ref[...], first) + mm(decay_ref[...], second)).astype(BF16)


def join_weights(head, query, key, value, strength, decay):
    depth = query.shape[0]
    step = depth // 4
    tall = lambda x: pl.BlockSpec((step, x.shape[1]), lambda i: (i, 0))
    return pl.pallas_call(
        weights_kernel,
        grid=(4,),
        out_shape=jax.ShapeDtypeStruct((depth, 4 * HEAD), BF16),
        in_specs=[pl.BlockSpec(memory_space=pltpu.SMEM)] + [tall(x) for x in (query, key, value, strength, decay)],
        out_specs=pl.BlockSpec((step, 4 * HEAD), lambda i: (i, 0)),
        cost_estimate=pl.CostEstimate(flops=10**8, bytes_accessed=depth * HEAD * 16, transcendentals=0),
    )(head, query, key, value, strength, decay)


def span_kernel(count, scal_ref, rows_ref, w_ref, extra_ref, g_ref, h_ref, ab_ref, proj, low, high, lasts):
    proj[...] = lax.dot_general(rows_ref[...], w_ref[...], NN, preferred_element_type=F32)
    row = lax.broadcasted_iota(jnp.int32, (BLOCK, BLOCK), 0)
    col = lax.broadcasted_iota(jnp.int32, (BLOCK, BLOCK), 1)
    upper = (row <= col).astype(F32)
    speed, largest = scal_ref[0], scal_ref[1]
    start = pl.program_id(0) * count
    mats, keep = [], []
    for b in range(count):
        at = slice(b * BLOCK, (b + 1) * BLOCK)
        q = silu(proj[at, 0:HEAD])
        k = silu(proj[at, HEAD : 2 * HEAD])
        v = silu(proj[at, 2 * HEAD : 3 * HEAD])
        k = k * lax.rsqrt(jnp.sum(k * k, axis=1, keepdims=True) + 1e-06)
        small = proj[at, 3 * HEAD : 4 * HEAD]
        strength = largest * (1.0 / (1.0 + jnp.exp(-small[:, 0:1])))
        flipped = small.T
        x = flipped[0:8, :]
        soft = jnp.maximum(x, 0.0) + jnp.log1p(jnp.exp(-jnp.abs(x)))
        steps = extra_ref[pl.ds(start + b, 1), :] - speed * soft[1:2, :]
        cum_row = lax.dot_general(
            jnp.broadcast_to(steps, (8, BLOCK)), upper, NN, preferred_element_type=F32, precision=lax.Precision.HIGHEST
        )[0:1, :]
        across = jnp.broadcast_to(cum_row, (BLOCK, BLOCK))
        down = across.T
        total = jnp.broadcast_to(cum_row[:, BLOCK - 1 : BLOCK], (BLOCK, BLOCK))
        decay = jnp.exp(jnp.where(row >= col, down - across, -1e30))
        grow = jnp.exp(down)
        both = mm(jnp.concatenate([k, q], axis=0), k, NT)
        mats.append(jnp.where(row > col, both[:BLOCK] * decay * strength, 0.0))
        right = jnp.concatenate([v * strength, k * (grow * strength)], axis=1)
        keep.append((q * grow, both[BLOCK:] * decay, right, k * jnp.exp(total - down)))
        lasts[start + b] = jnp.exp(total[0:8, :])
    invs = invert_unit_lower(mats, row, col)
    for b in range(count):
        query_dec, scores, right, keys_dec = keep[b]
        solved = mm(invs[b], right)
        seen = mm(scores, solved)
        kept = mm(keys_dec, solved, TN)
        high[start + b, :, :HEAD] = kept[:, :HEAD]
        high[start + b, :, HEAD:] = seen[:, :HEAD]
        low[start + b, :HEAD, :] = (query_dec - seen[:, HEAD:]).astype(BF16)
        low[start + b, HEAD:, :] = kept[:, HEAD:].astype(BF16)

    @pl.when(pl.program_id(0) == pl.num_programs(0) - 1)
    def _():
        maps = (row == col).astype(F32)
        memory = jnp.zeros((HEAD, HEAD), F32)
        for j in range(low.shape[0]):
            both = jnp.concatenate([maps, memory], axis=1).astype(BF16)
            out = mm(low[j], both)
            g_ref[j * BLOCK : (j + 1) * BLOCK, :] = out[:HEAD, :HEAD].astype(BF16)
            h_ref[j * BLOCK : (j + 1) * BLOCK, :] = out[:HEAD, HEAD:] + high[j, :, HEAD:]
            last = lasts[j, 0:1, :]
            maps = maps * last - out[HEAD:, :HEAD]
            memory = memory * last - out[HEAD:, HEAD:] + high[j, :, :HEAD]
        ab_ref[:, :HEAD] = maps.astype(BF16)
        ab_ref[:, HEAD:] = memory.astype(BF16)


def span_terms(scal, rows, weights, extra, count):
    length, depth = rows.shape
    blocks = length // BLOCK
    width = weights.shape[1]
    whole = lambda i: (0, 0)
    return pl.pallas_call(
        functools.partial(span_kernel, count),
        grid=(blocks // count,),
        out_shape=(
            jax.ShapeDtypeStruct((length, HEAD), BF16),
            jax.ShapeDtypeStruct((length, HEAD), F32),
            jax.ShapeDtypeStruct((HEAD, 2 * HEAD), BF16),
        ),
        in_specs=[
            pl.BlockSpec(memory_space=pltpu.SMEM),
            pl.BlockSpec((count * BLOCK, depth), lambda i: (i, 0)),
            pl.BlockSpec(weights.shape, whole),
            pl.BlockSpec(extra.shape, whole),
        ],
        out_specs=(
            pl.BlockSpec((length, HEAD), whole),
            pl.BlockSpec((length, HEAD), whole),
            pl.BlockSpec((HEAD, 2 * HEAD), whole),
        ),
        scratch_shapes=[
            pltpu.VMEM((count * BLOCK, width), F32),
            pltpu.VMEM((blocks, 2 * HEAD, HEAD), BF16),
            pltpu.VMEM((blocks, HEAD, 2 * HEAD), F32),
            pltpu.VMEM((blocks, 8, HEAD), F32),
        ],
        cost_estimate=pl.CostEstimate(
            flops=length * 2 * (depth * width + 40 * HEAD * HEAD * 4),
            bytes_accessed=2 * (rows.size + weights.size) + length * HEAD * 6,
            transcendentals=0,
        ),
    )(scal, rows, weights, extra)


def row_kernel(here_ref, own_ref, one_ref, two_ref, three_ref, before_ref, total_ref, slots):
    here = here_ref[0]
    slots[here] = own_ref[...]
    slots[(here + 3) % 4] = one_ref[...]
    slots[(here + 2) % 4] = two_ref[...]
    slots[(here + 1) % 4] = three_ref[...]
    row = lax.broadcasted_iota(jnp.int32, (HEAD, 2 * HEAD), 0)
    col = lax.broadcasted_iota(jnp.int32, (HEAD, 2 * HEAD), 1)
    eye = (row == col).astype(F32)
    so_far = slots[0].astype(F32)
    before = jnp.where(here == 0, eye, so_far)
    for k in range(1, 4):
        piece = slots[k]
        own = jnp.where(col >= HEAD, piece.astype(F32), 0.0)
        so_far = mm(piece[:, :HEAD], so_far) + own
        if k < 3:
            before = jnp.where(here > k, so_far, before)
    before_ref[...] = before
    total_ref[...] = so_far.astype(BF16)


def compose_row(here, own, one, two, three):
    vmem = pl.BlockSpec(memory_space=pltpu.VMEM)
    return pl.pallas_call(
        row_kernel,
        out_shape=(jax.ShapeDtypeStruct((HEAD, 2 * HEAD), F32), jax.ShapeDtypeStruct((HEAD, 2 * HEAD), BF16)),
        in_specs=[pl.BlockSpec(memory_space=pltpu.SMEM)] + [vmem] * 4,
        out_specs=(vmem, vmem),
        scratch_shapes=[pltpu.VMEM((4, HEAD, 2 * HEAD), BF16)],
        compiler_params=pltpu.CompilerParams(vmem_limit_bytes=8 * 1024 * 1024),
        cost_estimate=pl.CostEstimate(flops=12 * HEAD**3, bytes_accessed=8 * HEAD * HEAD, transcendentals=0),
    )(here, own, one, two, three)


def apply_kernel(here_ref, one_ref, two_ref, three_ref, before_ref, g_ref, h_ref, gain_ref, out_ref, slots):
    here = here_ref[0]
    slots[(here + 3) % 4] = one_ref[...]
    slots[(here + 2) % 4] = two_ref[...]
    slots[(here + 1) % 4] = three_ref[...]
    memory = jnp.where(here > 0, slots[0][:, HEAD:].astype(F32), 0.0)
    for k in range(1, 3):
        piece = slots[k]
        moved = mm(piece[:, :HEAD], memory) + piece[:, HEAD:].astype(F32)
        memory = jnp.where(here > k, moved, memory)
    memory = mm(before_ref[:, :HEAD], memory) + before_ref[:, HEAD:]
    heads_out = mm(g_ref[...], memory) + h_ref[...]
    scale = lax.rsqrt(jnp.mean(heads_out * heads_out, axis=1, keepdims=True) + norm_eps)
    out_ref[...] = (heads_out * scale * gain_ref[...]).astype(BF16)


def apply_memory(here, one, two, three, before, g, h, gain):
    vmem = pl.BlockSpec(memory_space=pltpu.VMEM)
    return pl.pallas_call(
        apply_kernel,
        out_shape=jax.ShapeDtypeStruct(h.shape, BF16),
        in_specs=[pl.BlockSpec(memory_space=pltpu.SMEM)] + [vmem] * 7,
        out_specs=vmem,
        scratch_shapes=[pltpu.VMEM((4, HEAD, 2 * HEAD), BF16)],
        compiler_params=pltpu.CompilerParams(vmem_limit_bytes=8 * 1024 * 1024),
        cost_estimate=pl.CostEstimate(flops=h.size * 2 * HEAD, bytes_accessed=h.size * 8, transcendentals=0),
    )(here, one, two, three, before, g, h, gain.reshape(1, HEAD))


def output_kernel(core_ref, x_ref, w_ref, mine_ref, theirs_ref, total):
    step = pl.program_id(0)

    @pl.when(step == 0)
    def _():
        total[...] = jnp.zeros_like(total)

    rows = jnp.concatenate([x_ref[0], x_ref[1]], axis=1)
    total[...] += mm(rows, w_ref[...])

    @pl.when(step == pl.num_programs(0) - 1)
    def _():
        first = core_ref[0] == 0
        mine_ref[...] = jnp.where(first, total[:BLOCK], total[BLOCK:])
        theirs_ref[...] = jnp.where(first, total[BLOCK:], total[:BLOCK]).astype(BF16)


def output_product(core, by_head, weights):
    depth, width = weights.shape
    whole = lambda i: (0, 0)
    return pl.pallas_call(
        output_kernel,
        grid=(depth // (2 * HEAD),),
        out_shape=(jax.ShapeDtypeStruct((BLOCK, width), F32), jax.ShapeDtypeStruct((BLOCK, width), BF16)),
        in_specs=[
            pl.BlockSpec(memory_space=pltpu.SMEM),
            pl.BlockSpec((2, 2 * BLOCK, HEAD), lambda i: (i, 0, 0)),
            pl.BlockSpec((2 * HEAD, width), lambda i: (i, 0)),
        ],
        out_specs=(pl.BlockSpec((BLOCK, width), whole), pl.BlockSpec((BLOCK, width), whole)),
        scratch_shapes=[pltpu.VMEM((2 * BLOCK, width), F32)],
        cost_estimate=pl.CostEstimate(
            flops=4 * BLOCK * depth * width, bytes_accessed=2 * depth * width, transcendentals=0
        ),
    )(core, by_head.reshape(-1, 2 * BLOCK, HEAD), weights)


def route_columns(side, experts):
    tokens = side.shape[1]
    expert = lax.broadcasted_iota(jnp.int32, (experts, tokens), 0).astype(F32)
    first, second = side[0:1] == expert, side[1:2] == expert
    named = (first | second).astype(F32)
    row = lax.broadcasted_iota(jnp.int32, (tokens, tokens), 0)
    col = lax.broadcasted_iota(jnp.int32, (tokens, tokens), 1)
    earlier = ((row < col) & (row // TOKENS == col // TOKENS)).astype(F32)
    return first, named, mm(named, earlier)


def slot_rows(named, slots, e):
    tokens = named.shape[1]
    rows = tokens // TOKENS * SLOTS
    row = lax.broadcasted_iota(jnp.int32, (rows, tokens), 0)
    col = lax.broadcasted_iota(jnp.int32, (rows, tokens), 1)
    taken = jnp.where(named[e : e + 1] > 0.5, slots[e : e + 1], -1.0)
    return (taken == (row % SLOTS).astype(F32)) & (row // SLOTS == col // TOKENS)


def pack_kernel(experts, tok_ref, out_ref):
    width = out_ref.shape[1]
    side = tok_ref[:, width:].astype(F32).T
    _, named, slots = route_columns(side, experts)
    rows = out_ref.shape[0] // experts
    group = 4
    for e in range(0, experts, group):
        pick = jnp.concatenate([slot_rows(named, slots, e + i).astype(F32) for i in range(group)], axis=0)
        out_ref[e * rows : (e + group) * rows, :] = mm(pick, tok_ref[:, :width]).astype(BF16)


def pack_tokens(tokens, experts):
    count, width = tokens.shape
    vmem = pl.BlockSpec(memory_space=pltpu.VMEM)
    rows = count // TOKENS * SLOTS * experts
    return pl.pallas_call(
        functools.partial(pack_kernel, experts),
        out_shape=jax.ShapeDtypeStruct((rows, width - HEAD), BF16),
        in_specs=[vmem],
        out_specs=vmem,
        cost_estimate=pl.CostEstimate(flops=2 * rows * count * width, bytes_accessed=2 * rows * width, transcendentals=0),
    )(tokens)


def combine_kernel(experts, core_ref, side_ref, back_ref, mine_ref, theirs_ref, total):
    side = side_ref[...].astype(F32).T
    first, named, slots = route_columns(side, experts)
    share = [side[2 + k : 3 + k] + side[4 + k : 5 + k] + side[6 + k : 7 + k] for k in range(2)]
    picks = []
    for e in range(experts):
        share_row = jnp.where(first[e : e + 1], share[0], share[1])
        picks.append(jnp.where(slot_rows(named, slots, e), share_row, 0.0))
    pick = jnp.concatenate(picks, axis=0)
    high = pick.astype(BF16)
    low = (pick - high.astype(F32)).astype(BF16)
    back = back_ref[...]
    out = mm(high, back, TN) + mm(low, back, TN)
    total[...] = out.reshape(total.shape)
    core = core_ref[0]
    for z in range(mine_ref.shape[0]):
        mine_ref[z] = total[2 * z + core].astype(BF16)
        theirs_ref[z] = total[2 * z + 1 - core].astype(BF16)


def combine_tokens(core, tokens, back, experts):
    count, _ = tokens.shape
    width = back.shape[1]
    devices = count // TOKENS
    whole = lambda i: (0, 0)
    cube = lambda i: (0, 0, 0)
    half = (devices // 2, TOKENS, width)
    out = jax.ShapeDtypeStruct(half, BF16)
    return pl.pallas_call(
        functools.partial(combine_kernel, experts),
        grid=(1,),
        out_shape=(out, out),
        in_specs=[
            pl.BlockSpec(memory_space=pltpu.SMEM),
            pl.BlockSpec((count, HEAD), lambda i: (0, width // HEAD)),
            pl.BlockSpec(back.shape, whole),
        ],
        out_specs=(pl.BlockSpec(half, cube), pl.BlockSpec(half, cube)),
        scratch_shapes=[pltpu.VMEM((devices, TOKENS, width), F32)],
        cost_estimate=pl.CostEstimate(
            flops=4 * count * back.size, bytes_accessed=2 * back.size + 4 * count * width, transcendentals=0
        ),
    )(core, tokens, back)


def expert_kernel(rows_ref, gate_ref, up_ref, down_ref, out_ref, rows, gate, up, down, sems):
    copies = [
        pltpu.make_async_copy(src, dst, sems.at[i])
        for i, (src, dst) in enumerate(((rows_ref, rows), (gate_ref, gate), (up_ref, up), (down_ref, down)))
    ]
    for copy in copies:
        copy.start()
    copies[0].wait()
    copies[1].wait()
    gated = silu(mm(rows[...], gate[...], NT))
    copies[2].wait()
    hidden = (gated * mm(rows[...], up[...], NT)).astype(BF16)
    copies[3].wait()
    out_ref[...] = mm(hidden, down[...]).astype(BF16)


def expert_sums(rows, gate, up, down):
    count, width = rows.shape
    units = gate.shape[0]
    return pl.pallas_call(
        expert_kernel,
        out_shape=jax.ShapeDtypeStruct((count, width), BF16),
        in_specs=[pl.BlockSpec(memory_space=pl.ANY)] * 4,
        out_specs=pl.BlockSpec(memory_space=pltpu.VMEM),
        scratch_shapes=[
            pltpu.VMEM((count, width), BF16),
            pltpu.VMEM((units, width), BF16),
            pltpu.VMEM((units, width), BF16),
            pltpu.VMEM((units, width), BF16),
            pltpu.SemaphoreType.DMA((4,)),
        ],
        cost_estimate=pl.CostEstimate(
            flops=6 * count * width * units, bytes_accessed=6 * units * width + 4 * count * width, transcendentals=0
        ),
    )(rows, gate, up, down)


def around(x, axis):
    size = lax.axis_size(axis)
    out = []
    for k in range(1, size):
        out.append(lax.ppermute(x, axis, [(i, (i + k) % size) for i in range(size)]))
    return out


def mixed_step(
    mixer_input_rows,
    mixer_norm_gain,
    query_weight,
    key_weight,
    value_weight,
    write_strength_projection,
    decay_projection,
    head_decay_speed,
    largest_write_strength,
    extra_log_decay,
    head_norm_gain,
    mixer_output_weight,
    expert_input_rows,
    expert_norm_gain,
    routes,
    expert_route_weight,
    gate_weight,
    up_weight,
    down_weight,
):
    head = lax.axis_index(TP)
    core = lax.axis_index("tp_1")
    experts = gate_weight.shape[0] * lax.axis_size(EP)
    cross = lambda x: lax.ppermute(x, "tp_1", [(0, 1), (1, 0)])

    mix_normed = rms_scale(mixer_input_rows, mixer_norm_gain)
    mix_rows = lax.all_gather(mix_normed, TP, axis=0, tiled=True)

    exp_normed = rms_scale(expert_input_rows, expert_norm_gain)
    parts, rest = [], expert_route_weight
    for _ in range(3):
        part = lax.reduce_precision(rest, 8, 7)
        parts.append(part.astype(BF16))
        rest = rest - part
    side = jnp.concatenate([routes.astype(BF16)] + parts, axis=1)
    side = jnp.pad(side, ((0, 0), (0, HEAD - side.shape[1])))
    tokens = lax.all_gather(jnp.concatenate([exp_normed, side], axis=1), TP, axis=0, tiled=True)
    packed = pack_tokens(tokens, experts)
    exp_rows = lax.all_to_all(packed, EP, split_axis=0, concat_axis=0, tiled=True)
    partial = expert_sums(exp_rows, gate_weight[0].T, up_weight[0].T, down_weight[0])
    back = lax.all_to_all(partial, EP, split_axis=0, concat_axis=0, tiled=True)
    mine, theirs = combine_tokens(core[None], tokens, back, experts)
    crossed = cross(theirs)
    pair = (mine.astype(F32) + crossed.astype(F32)).astype(BF16)

    weights = join_weights(
        head[None], query_weight, key_weight, value_weight, write_strength_projection, decay_projection
    )
    scal = jnp.concatenate([head_decay_speed, largest_write_strength])
    extra = extra_log_decay.reshape(-1, BLOCK)
    gains, local, span = span_terms(scal, mix_rows, weights, extra, 8)
    before, total = compose_row(lax.axis_index("ep_1")[None], span, *around(span, "ep_1"))
    mixed = apply_memory(lax.axis_index("ep_0")[None], *around(total, "ep_0"), before, gains, local, head_norm_gain)

    by_head = lax.all_to_all(mixed, "tp_0", split_axis=0, concat_axis=0, tiled=True)
    w_own = lax.all_gather(mixer_output_weight, "tp_0", axis=0, tiled=True)
    mix_mine, mix_theirs = output_product(core[None], by_head, w_own)
    mix_out = (mix_mine + cross(mix_theirs).astype(F32)).astype(BF16)

    pieces = lax.all_to_all(pair, "tp_0", split_axis=0, concat_axis=0, tiled=True)
    exp_out = jnp.sum(pieces.astype(F32), axis=0).astype(BF16)
    return (mix_out, exp_out)


def solution(mesh):
    torus = Mesh(mesh.devices.reshape(4, 4, 8, 2), ("ep_0", "ep_1", "tp_0", "tp_1"))
    placed = (
        P(EP_TP, None),
        P(),
        P(None, TP),
        P(None, TP),
        P(None, TP),
        P(),
        P(),
        P(TP),
        P(TP),
        P(EP, TP),
        P(),
        P(TP, None),
        P(EP_TP, None),
        P(),
        P(EP_TP, None),
        P(EP_TP, None),
        P(EP, None, TP),
        P(EP, None, TP),
        P(EP, TP, None),
    )
    return jax.shard_map(
        mixed_step,
        mesh=torus,
        in_specs=placed,
        out_specs=(P(EP_TP, None), P(EP_TP, None)),
        check_vma=False,
    )
```

```python
import functools

import jax
import jax.numpy as jnp
from jax import lax
from jax.experimental import pallas as pl
from jax.experimental.pallas import tpu as pltpu
from jax.sharding import Mesh
from jax.sharding import PartitionSpec as P


HEAD = 128
BLOCK = 128
TOKENS = 8
SLOTS = 2
EP = ("ep_0", "ep_1")
TP = ("tp_0", "tp_1")
EP_TP = ("ep_0", "ep_1", "tp_0", "tp_1")
F32 = jnp.float32
BF16 = jnp.bfloat16


norm_eps = 1e-06
NN = (((1,), (0,)), ((), ()))
NT = (((1,), (1,)), ((), ()))
TN = (((0,), (0,)), ((), ()))


def mm(a, b, dims=NN):
    return lax.dot_general(a.astype(BF16), b.astype(BF16), dims, preferred_element_type=F32)


def silu(x):
    return x / (1.0 + jnp.exp(-x))


def rms_scale(rows_in, gain_vec):
    widened = rows_in.astype(F32)
    scaled = widened * lax.rsqrt(jnp.mean(widened * widened, axis=-1, keepdims=True) + norm_eps)
    return (scaled * gain_vec).astype(BF16)


def invert_unit_lower(mats, row, col):
    apart = row ^ col
    eye = (row == col).astype(F32)
    size = 1
    invs = None
    while size < BLOCK:
        pick = (apart >= size) & (apart < 2 * size)
        parts = [jnp.where(pick, m, 0.0) for m in mats]
        if invs is None:
            invs = [eye - p for p in parts]
        else:
            invs_low = [x.astype(BF16) for x in invs]
            half = [mm(p, x) for p, x in zip(parts, invs_low)]
            invs = [x - mm(xl, h) for x, xl, h in zip(invs, invs_low, half)]
        size *= 2
    return invs


def weights_kernel(head_ref, q_ref, k_ref, v_ref, strength_ref, decay_ref, out_ref):
    out_ref[:, 0:HEAD] = q_ref[...]
    out_ref[:, HEAD : 2 * HEAD] = k_ref[...]
    out_ref[:, 2 * HEAD : 3 * HEAD] = v_ref[...]
    heads = strength_ref.shape[1]
    row = lax.broadcasted_iota(jnp.int32, (heads, HEAD), 0)
    col = lax.broadcasted_iota(jnp.int32, (heads, HEAD), 1)
    here = row == head_ref[0]
    first = (here & (col == 0)).astype(BF16)
    second = (here & (col == 1)).astype(BF16)
    out_ref[:, 3 * HEAD :] = (mm(strength_ref[...], first) + mm(decay_ref[...], second)).astype(BF16)


def join_weights(head, query, key, value, strength, decay):
    depth = query.shape[0]
    step = depth // 4
    tall = lambda x: pl.BlockSpec((step, x.shape[1]), lambda i: (i, 0))
    return pl.pallas_call(
        weights_kernel,
        grid=(4,),
        out_shape=jax.ShapeDtypeStruct((depth, 4 * HEAD), BF16),
        in_specs=[pl.BlockSpec(memory_space=pltpu.SMEM)] + [tall(x) for x in (query, key, value, strength, decay)],
        out_specs=pl.BlockSpec((step, 4 * HEAD), lambda i: (i, 0)),
        cost_estimate=pl.CostEstimate(flops=10**8, bytes_accessed=depth * HEAD * 16, transcendentals=0),
    )(head, query, key, value, strength, decay)


def span_kernel(count, scal_ref, rows_ref, w_ref, extra_ref, g_ref, h_ref, ab_ref, proj, low, high, lasts):
    proj[...] = lax.dot_general(rows_ref[...], w_ref[...], NN, preferred_element_type=F32)
    row = lax.broadcasted_iota(jnp.int32, (BLOCK, BLOCK), 0)
    col = lax.broadcasted_iota(jnp.int32, (BLOCK, BLOCK), 1)
    upper = (row <= col).astype(F32)
    speed, largest = scal_ref[0], scal_ref[1]
    start = pl.program_id(0) * count
    mats, keep = [], []
    for b in range(count):
        at = slice(b * BLOCK, (b + 1) * BLOCK)
        q = silu(proj[at, 0:HEAD])
        k = silu(proj[at, HEAD : 2 * HEAD])
        v = silu(proj[at, 2 * HEAD : 3 * HEAD])
        k = k * lax.rsqrt(jnp.sum(k * k, axis=1, keepdims=True) + 1e-06)
        small = proj[at, 3 * HEAD : 4 * HEAD]
        strength = largest * (1.0 / (1.0 + jnp.exp(-small[:, 0:1])))
        flipped = small.T
        x = flipped[0:8, :]
        soft = jnp.maximum(x, 0.0) + jnp.log1p(jnp.exp(-jnp.abs(x)))
        steps = extra_ref[pl.ds(start + b, 1), :] - speed * soft[1:2, :]
        cum_row = lax.dot_general(
            jnp.broadcast_to(steps, (8, BLOCK)), upper, NN, preferred_element_type=F32, precision=lax.Precision.HIGHEST
        )[0:1, :]
        across = jnp.broadcast_to(cum_row, (BLOCK, BLOCK))
        down = across.T
        total = jnp.broadcast_to(cum_row[:, BLOCK - 1 : BLOCK], (BLOCK, BLOCK))
        decay = jnp.exp(jnp.where(row >= col, down - across, -1e30))
        grow = jnp.exp(down)
        both = mm(jnp.concatenate([k, q], axis=0), k, NT)
        mats.append(jnp.where(row > col, both[:BLOCK] * decay * strength, 0.0))
        right = jnp.concatenate([v * strength, k * (grow * strength)], axis=1)
        keep.append((q * grow, both[BLOCK:] * decay, right, k * jnp.exp(total - down)))
        lasts[start + b] = jnp.exp(total[0:8, :])
    invs = invert_unit_lower(mats, row, col)
    for b in range(count):
        query_dec, scores, right, keys_dec = keep[b]
        solved = mm(invs[b], right)
        seen = mm(scores, solved)
        kept = mm(keys_dec, solved, TN)
        high[start + b, :, :HEAD] = kept[:, :HEAD]
        high[start + b, :, HEAD:] = seen[:, :HEAD]
        low[start + b, :HEAD, :] = (query_dec - seen[:, HEAD:]).astype(BF16)
        low[start + b, HEAD:, :] = kept[:, HEAD:].astype(BF16)

    @pl.when(pl.program_id(0) == pl.num_programs(0) - 1)
    def _():
        maps = (row == col).astype(F32)
        memory = jnp.zeros((HEAD, HEAD), F32)
        for j in range(low.shape[0]):
            both = jnp.concatenate([maps, memory], axis=1).astype(BF16)
            out = mm(low[j], both)
            g_ref[j * BLOCK : (j + 1) * BLOCK, :] = out[:HEAD, :HEAD].astype(BF16)
            h_ref[j * BLOCK : (j + 1) * BLOCK, :] = out[:HEAD, HEAD:] + high[j, :, HEAD:]
            last = lasts[j, 0:1, :]
            maps = maps * last - out[HEAD:, :HEAD]
            memory = memory * last - out[HEAD:, HEAD:] + high[j, :, :HEAD]
        ab_ref[:, :HEAD] = maps.astype(BF16)
        ab_ref[:, HEAD:] = memory.astype(BF16)


def span_terms(scal, rows, weights, extra, count):
    length, depth = rows.shape
    blocks = length // BLOCK
    width = weights.shape[1]
    whole = lambda i: (0, 0)
    return pl.pallas_call(
        functools.partial(span_kernel, count),
        grid=(blocks // count,),
        out_shape=(
            jax.ShapeDtypeStruct((length, HEAD), BF16),
            jax.ShapeDtypeStruct((length, HEAD), F32),
            jax.ShapeDtypeStruct((HEAD, 2 * HEAD), BF16),
        ),
        in_specs=[
            pl.BlockSpec(memory_space=pltpu.SMEM),
            pl.BlockSpec((count * BLOCK, depth), lambda i: (i, 0)),
            pl.BlockSpec(weights.shape, whole),
            pl.BlockSpec(extra.shape, whole),
        ],
        out_specs=(
            pl.BlockSpec((length, HEAD), whole),
            pl.BlockSpec((length, HEAD), whole),
            pl.BlockSpec((HEAD, 2 * HEAD), whole),
        ),
        scratch_shapes=[
            pltpu.VMEM((count * BLOCK, width), F32),
            pltpu.VMEM((blocks, 2 * HEAD, HEAD), BF16),
            pltpu.VMEM((blocks, HEAD, 2 * HEAD), F32),
            pltpu.VMEM((blocks, 8, HEAD), F32),
        ],
        cost_estimate=pl.CostEstimate(
            flops=length * 2 * (depth * width + 40 * HEAD * HEAD * 4),
            bytes_accessed=2 * (rows.size + weights.size) + length * HEAD * 6,
            transcendentals=0,
        ),
    )(scal, rows, weights, extra)


def row_kernel(here_ref, own_ref, one_ref, two_ref, three_ref, before_ref, total_ref, slots):
    here = here_ref[0]
    slots[here] = own_ref[...]
    slots[(here + 3) % 4] = one_ref[...]
    slots[(here + 2) % 4] = two_ref[...]
    slots[(here + 1) % 4] = three_ref[...]
    row = lax.broadcasted_iota(jnp.int32, (HEAD, 2 * HEAD), 0)
    col = lax.broadcasted_iota(jnp.int32, (HEAD, 2 * HEAD), 1)
    eye = (row == col).astype(F32)
    so_far = slots[0].astype(F32)
    before = jnp.where(here == 0, eye, so_far)
    for k in range(1, 4):
        piece = slots[k]
        own = jnp.where(col >= HEAD, piece.astype(F32), 0.0)
        so_far = mm(piece[:, :HEAD], so_far) + own
        if k < 3:
            before = jnp.where(here > k, so_far, before)
    before_ref[...] = before
    total_ref[...] = so_far.astype(BF16)


def compose_row(here, own, one, two, three):
    vmem = pl.BlockSpec(memory_space=pltpu.VMEM)
    return pl.pallas_call(
        row_kernel,
        out_shape=(jax.ShapeDtypeStruct((HEAD, 2 * HEAD), F32), jax.ShapeDtypeStruct((HEAD, 2 * HEAD), BF16)),
        in_specs=[pl.BlockSpec(memory_space=pltpu.SMEM)] + [vmem] * 4,
        out_specs=(vmem, vmem),
        scratch_shapes=[pltpu.VMEM((4, HEAD, 2 * HEAD), BF16)],
        compiler_params=pltpu.CompilerParams(vmem_limit_bytes=8 * 1024 * 1024),
        cost_estimate=pl.CostEstimate(flops=12 * HEAD**3, bytes_accessed=8 * HEAD * HEAD, transcendentals=0),
    )(here, own, one, two, three)


def apply_kernel(here_ref, one_ref, two_ref, three_ref, before_ref, g_ref, h_ref, gain_ref, out_ref, slots, entering):
    @pl.when(pl.program_id(0) == 0)
    def _():
        here = here_ref[0]
        slots[(here + 3) % 4] = one_ref[...]
        slots[(here + 2) % 4] = two_ref[...]
        slots[(here + 1) % 4] = three_ref[...]
        memory = jnp.where(here > 0, slots[0][:, HEAD:].astype(F32), 0.0)
        for k in range(1, 3):
            piece = slots[k]
            moved = mm(piece[:, :HEAD], memory) + piece[:, HEAD:].astype(F32)
            memory = jnp.where(here > k, moved, memory)
        entering[...] = mm(before_ref[:, :HEAD], memory) + before_ref[:, HEAD:]

    heads_out = mm(g_ref[...], entering[...]) + h_ref[...]
    scale = lax.rsqrt(jnp.mean(heads_out * heads_out, axis=1, keepdims=True) + norm_eps)
    out_ref[...] = (heads_out * scale * gain_ref[...]).astype(BF16)


def apply_memory(here, one, two, three, before, g, h, gain):
    rows = h.shape[0]
    step = rows // 4
    whole = lambda i: (0, 0)
    tall = lambda i: (i, 0)
    piece = pl.BlockSpec((HEAD, 2 * HEAD), whole)
    return pl.pallas_call(
        apply_kernel,
        grid=(4,),
        out_shape=jax.ShapeDtypeStruct(h.shape, BF16),
        in_specs=[pl.BlockSpec(memory_space=pltpu.SMEM)]
        + [piece] * 4
        + [pl.BlockSpec((step, HEAD), tall), pl.BlockSpec((step, HEAD), tall), pl.BlockSpec((1, HEAD), whole)],
        out_specs=pl.BlockSpec((step, HEAD), tall),
        scratch_shapes=[pltpu.VMEM((4, HEAD, 2 * HEAD), BF16), pltpu.VMEM((HEAD, HEAD), F32)],
        cost_estimate=pl.CostEstimate(flops=h.size * 2 * HEAD, bytes_accessed=h.size * 8, transcendentals=0),
    )(here, one, two, three, before, g, h, gain.reshape(1, HEAD))


def output_kernel(core_ref, x_ref, w_ref, mine_ref, theirs_ref, rows):
    @pl.when(pl.program_id(0) == 0)
    def _():
        for part in range(2):
            owner = core_ref[0] if part == 0 else 1 - core_ref[0]
            at = pl.ds(pl.multiple_of(owner * BLOCK, BLOCK), BLOCK)
            for h in range(x_ref.shape[0]):
                rows[part * BLOCK : (part + 1) * BLOCK, h * HEAD : (h + 1) * HEAD] = x_ref[h, at, :]

    out = mm(rows[...], w_ref[...])
    mine_ref[...] = out[:BLOCK]
    theirs_ref[...] = out[BLOCK:].astype(BF16)


def output_product(core, by_head, weights):
    depth, width = weights.shape
    heads = depth // HEAD
    step = width // 4
    column = lambda i: (0, i)
    return pl.pallas_call(
        output_kernel,
        grid=(4,),
        out_shape=(jax.ShapeDtypeStruct((BLOCK, width), F32), jax.ShapeDtypeStruct((BLOCK, width), BF16)),
        in_specs=[
            pl.BlockSpec(memory_space=pltpu.SMEM),
            pl.BlockSpec((heads, 2 * BLOCK, HEAD), lambda i: (0, 0, 0)),
            pl.BlockSpec((depth, step), column),
        ],
        out_specs=(pl.BlockSpec((BLOCK, step), column), pl.BlockSpec((BLOCK, step), column)),
        scratch_shapes=[pltpu.VMEM((2 * BLOCK, depth), BF16)],
        cost_estimate=pl.CostEstimate(
            flops=4 * BLOCK * depth * width, bytes_accessed=2 * depth * width, transcendentals=0
        ),
    )(core, by_head.reshape(heads, 2 * BLOCK, HEAD), weights)


def route_columns(side, experts):
    tokens = side.shape[1]
    expert = lax.broadcasted_iota(jnp.int32, (experts, tokens), 0).astype(F32)
    first, second = side[0:1] == expert, side[1:2] == expert
    named = (first | second).astype(F32)
    row = lax.broadcasted_iota(jnp.int32, (tokens, tokens), 0)
    col = lax.broadcasted_iota(jnp.int32, (tokens, tokens), 1)
    earlier = ((row < col) & (row // TOKENS == col // TOKENS)).astype(F32)
    return first, named, mm(named, earlier)


def slot_rows(named, slots, e):
    tokens = named.shape[1]
    rows = tokens // TOKENS * SLOTS
    row = lax.broadcasted_iota(jnp.int32, (rows, tokens), 0)
    col = lax.broadcasted_iota(jnp.int32, (rows, tokens), 1)
    taken = jnp.where(named[e : e + 1] > 0.5, slots[e : e + 1], -1.0)
    return (taken == (row % SLOTS).astype(F32)) & (row // SLOTS == col // TOKENS)


def pack_kernel(experts, tok_ref, out_ref):
    width = out_ref.shape[1]
    side = tok_ref[:, width:].astype(F32).T
    _, named, slots = route_columns(side, experts)
    rows = out_ref.shape[0] // experts
    group = 4
    for e in range(0, experts, group):
        pick = jnp.concatenate([slot_rows(named, slots, e + i).astype(F32) for i in range(group)], axis=0)
        out_ref[e * rows : (e + group) * rows, :] = mm(pick, tok_ref[:, :width]).astype(BF16)


def pack_tokens(tokens, experts):
    count, width = tokens.shape
    vmem = pl.BlockSpec(memory_space=pltpu.VMEM)
    rows = count // TOKENS * SLOTS * experts
    return pl.pallas_call(
        functools.partial(pack_kernel, experts),
        out_shape=jax.ShapeDtypeStruct((rows, width - HEAD), BF16),
        in_specs=[vmem],
        out_specs=vmem,
        cost_estimate=pl.CostEstimate(flops=2 * rows * count * width, bytes_accessed=2 * rows * width, transcendentals=0),
    )(tokens)


def combine_kernel(experts, side_ref, back_ref, out_ref):
    side = side_ref[...].astype(F32).T
    first, named, slots = route_columns(side, experts)
    share = [side[2 + k : 3 + k] + side[4 + k : 5 + k] + side[6 + k : 7 + k] for k in range(2)]
    picks = []
    for e in range(experts):
        share_row = jnp.where(first[e : e + 1], share[0], share[1])
        picks.append(jnp.where(slot_rows(named, slots, e), share_row, 0.0))
    pick = jnp.concatenate(picks, axis=0)
    high = pick.astype(BF16)
    low = (pick - high.astype(F32)).astype(BF16)
    back = back_ref[...]
    out = mm(high, back, TN) + mm(low, back, TN)
    out_ref[...] = out.reshape(out_ref.shape).astype(BF16)


def combine_tokens(tokens, back, experts):
    count, _ = tokens.shape
    width = back.shape[1]
    shape = (count // TOKENS, TOKENS, width)
    return pl.pallas_call(
        functools.partial(combine_kernel, experts),
        grid=(1,),
        out_shape=jax.ShapeDtypeStruct(shape, BF16),
        in_specs=[
            pl.BlockSpec((count, HEAD), lambda i: (0, width // HEAD)),
            pl.BlockSpec(back.shape, lambda i: (0, 0)),
        ],
        out_specs=pl.BlockSpec(shape, lambda i: (0, 0, 0)),
        cost_estimate=pl.CostEstimate(
            flops=4 * count * back.size, bytes_accessed=2 * back.size + 2 * count * width, transcendentals=0
        ),
    )(tokens, back)


def expert_kernel(own_ref, other_ref, gate_ref, up_ref, down_ref, mine_ref, theirs_ref, rows, gate, up, down, sems):
    half = own_ref.shape[0]
    pairs = (
        (own_ref, rows.at[pl.ds(0, half)]),
        (other_ref, rows.at[pl.ds(half, half)]),
        (gate_ref, gate),
        (up_ref, up),
        (down_ref, down),
    )
    copies = [pltpu.make_async_copy(src, dst, sems.at[i]) for i, (src, dst) in enumerate(pairs)]
    for copy in copies:
        copy.start()
    for copy in copies[:3]:
        copy.wait()
    gated = silu(mm(rows[...], gate[...], NT))
    copies[3].wait()
    hidden = (gated * mm(rows[...], up[...], NT)).astype(BF16)
    copies[4].wait()
    theirs_ref[...] = mm(hidden[half:], down[...]).astype(BF16)
    mine_ref[...] = mm(hidden[:half], down[...]).astype(BF16)


def expert_sums(own, other, gate, up, down):
    half, width = own.shape
    units = gate.shape[0]
    out = jax.ShapeDtypeStruct((half, width), BF16)
    vmem = pl.BlockSpec(memory_space=pltpu.VMEM)
    return pl.pallas_call(
        expert_kernel,
        out_shape=(out, out),
        in_specs=[pl.BlockSpec(memory_space=pl.ANY)] * 5,
        out_specs=(vmem, vmem),
        scratch_shapes=[
            pltpu.VMEM((2 * half, width), BF16),
            pltpu.VMEM((units, width), BF16),
            pltpu.VMEM((units, width), BF16),
            pltpu.VMEM((units, width), BF16),
            pltpu.SemaphoreType.DMA((5,)),
        ],
        cost_estimate=pl.CostEstimate(
            flops=12 * half * width * units, bytes_accessed=6 * units * width + 8 * half * width, transcendentals=0
        ),
    )(own, other, gate, up, down)


def around(x, axis):
    size = lax.axis_size(axis)
    out = []
    for k in range(1, size):
        out.append(lax.ppermute(x, axis, [(i, (i + k) % size) for i in range(size)]))
    return out


def mixed_step(
    mixer_input_rows,
    mixer_norm_gain,
    query_weight,
    key_weight,
    value_weight,
    write_strength_projection,
    decay_projection,
    head_decay_speed,
    largest_write_strength,
    extra_log_decay,
    head_norm_gain,
    mixer_output_weight,
    expert_input_rows,
    expert_norm_gain,
    routes,
    expert_route_weight,
    gate_weight,
    up_weight,
    down_weight,
):
    head = lax.axis_index(TP)
    core = lax.axis_index("tp_1")
    experts = gate_weight.shape[0] * lax.axis_size(EP)
    cross = lambda x: lax.ppermute(x, "tp_1", [(0, 1), (1, 0)])

    mix_normed = rms_scale(mixer_input_rows, mixer_norm_gain)
    mix_rows = lax.all_gather(mix_normed, TP, axis=0, tiled=True)

    exp_normed = rms_scale(expert_input_rows, expert_norm_gain)
    parts, rest = [], expert_route_weight
    for _ in range(3):
        part = lax.reduce_precision(rest, 8, 7)
        parts.append(part.astype(BF16))
        rest = rest - part
    side = jnp.concatenate([routes.astype(BF16)] + parts, axis=1)
    side = jnp.pad(side, ((0, 0), (0, HEAD - side.shape[1])))
    tokens = lax.all_gather(jnp.concatenate([exp_normed, side], axis=1), "tp_0", axis=0, tiled=True)
    packed = pack_tokens(tokens, experts)
    exp_rows = lax.all_to_all(packed, EP, split_axis=0, concat_axis=0, tiled=True)
    other_rows = cross(exp_rows)
    mine, theirs = expert_sums(exp_rows, other_rows, gate_weight[0].T, up_weight[0].T, down_weight[0])
    pair = (mine.astype(F32) + cross(theirs).astype(F32)).astype(BF16)
    back = lax.all_to_all(pair, EP, split_axis=0, concat_axis=0, tiled=True)
    combined = combine_tokens(tokens, back, experts)

    weights = join_weights(
        head[None], query_weight, key_weight, value_weight, write_strength_projection, decay_projection
    )
    scal = jnp.concatenate([head_decay_speed, largest_write_strength])
    extra = extra_log_decay.reshape(-1, BLOCK)
    gains, local, span = span_terms(scal, mix_rows, weights, extra, 8)
    row_pieces = around(span, "ep_1")
    before, total = compose_row(lax.axis_index("ep_1")[None], span, *row_pieces)
    mixed = apply_memory(lax.axis_index("ep_0")[None], *around(total, "ep_0"), before, gains, local, head_norm_gain)

    by_head = lax.all_to_all(mixed, "tp_0", split_axis=0, concat_axis=0, tiled=True)
    w_own = lax.all_gather(mixer_output_weight, "tp_0", axis=0, tiled=True)
    mix_mine, mix_theirs = output_product(core[None], by_head, w_own)
    mix_out = (mix_mine + cross(mix_theirs).astype(F32)).astype(BF16)

    pieces = lax.all_to_all(combined, "tp_0", split_axis=0, concat_axis=0, tiled=True)
    exp_out = jnp.sum(pieces.astype(F32), axis=0).astype(BF16)
    return (mix_out, exp_out)


def solution(mesh):
    torus = Mesh(mesh.devices.reshape(4, 4, 8, 2), ("ep_0", "ep_1", "tp_0", "tp_1"))
    placed = (
        P(EP_TP, None),
        P(),
        P(None, TP),
        P(None, TP),
        P(None, TP),
        P(),
        P(),
        P(TP),
        P(TP),
        P(EP, TP),
        P(),
        P(TP, None),
        P(EP_TP, None),
        P(),
        P(EP_TP, None),
        P(EP_TP, None),
        P(EP, None, TP),
        P(EP, None, TP),
        P(EP, TP, None),
    )
    return jax.shard_map(
        mixed_step,
        mesh=torus,
        in_specs=placed,
        out_specs=(P(EP_TP, None), P(EP_TP, None)),
        check_vma=False,
    )
```

```python
import functools

import jax
import jax.numpy as jnp
from jax import lax
from jax.experimental import pallas as pl
from jax.experimental.pallas import tpu as pltpu
from jax.sharding import Mesh
from jax.sharding import PartitionSpec as P


HEAD = 128
BLOCK = 128
TOKENS = 8
SLOTS = 2
SPAN_LIMIT = 44
EP = ("ep_0", "ep_1")
TP = ("tp_0", "tp_1")
EP_TP = ("ep_0", "ep_1", "tp_0", "tp_1")
F32 = jnp.float32
BF16 = jnp.bfloat16


norm_eps = 1e-06
NN = (((1,), (0,)), ((), ()))
NT = (((1,), (1,)), ((), ()))
TN = (((0,), (0,)), ((), ()))


def mm(a, b, dims=NN):
    return lax.dot_general(a.astype(BF16), b.astype(BF16), dims, preferred_element_type=F32)


def silu(x):
    return x / (1.0 + jnp.exp(-x))


def rms_scale(rows_in, gain_vec):
    widened = rows_in.astype(F32)
    scaled = widened * lax.rsqrt(jnp.mean(widened * widened, axis=-1, keepdims=True) + norm_eps)
    return (scaled * gain_vec).astype(BF16)


def invert_unit_lower(mats, row, col):
    apart = row ^ col
    eye = (row == col).astype(F32)
    size = 1
    invs = None
    while size < BLOCK:
        pick = (apart >= size) & (apart < 2 * size)
        parts = [jnp.where(pick, m, 0.0) for m in mats]
        if invs is None:
            invs = [eye - p for p in parts]
        else:
            invs_low = [x.astype(BF16) for x in invs]
            half = [mm(p, x) for p, x in zip(parts, invs_low)]
            invs = [x - mm(xl, h) for x, xl, h in zip(invs, invs_low, half)]
        size *= 2
    return invs


def span_kernel(
    chunks, scal_ref, head_ref, rows_ref, q_ref, k_ref, v_ref, strength_ref, decay_ref, extra_ref,
    g_ref, h_ref, ab_ref, rows, weights, proj, low, high, lasts, sems
):
    tall = rows_ref.shape[0] // chunks
    blocks = rows_ref.shape[0] // BLOCK
    count = blocks // 2
    copies = [
        pltpu.make_async_copy(ref, weights.at[:, pl.ds(i * HEAD, HEAD)], sems.at[i])
        for i, ref in enumerate((q_ref, k_ref, v_ref))
    ]
    row_copies = [
        pltpu.make_async_copy(rows_ref.at[pl.ds(i * tall, tall)], rows.at[pl.ds(i * tall, tall)], sems.at[3 + i])
        for i in range(chunks)
    ]
    for copy in copies + row_copies:
        copy.start()
    heads = strength_ref.shape[0]
    pick_row = lax.broadcasted_iota(jnp.int32, (heads, HEAD), 0) == head_ref[0]
    pick_col = lax.broadcasted_iota(jnp.int32, (heads, HEAD), 1)
    weights[:, 3 * HEAD :] = (
        mm(strength_ref[...], (pick_row & (pick_col == 0)).astype(BF16), TN)
        + mm(decay_ref[...], (pick_row & (pick_col == 1)).astype(BF16), TN)
    ).astype(BF16)
    row = lax.broadcasted_iota(jnp.int32, (BLOCK, BLOCK), 0)
    col = lax.broadcasted_iota(jnp.int32, (BLOCK, BLOCK), 1)
    upper = (row <= col).astype(F32)
    speed, largest = scal_ref[0], scal_ref[1]
    for copy in copies:
        copy.wait()

    def half(i, carry):
        start = i * count
        for c in range(chunks // 2):
            chunk = i * (chunks // 2) + c
            at = pl.ds(pl.multiple_of(chunk * tall, tall), tall)
            pltpu.make_async_copy(rows_ref.at[at], rows.at[at], sems.at[3 + chunk]).wait()
            proj[c * tall : (c + 1) * tall, :] = lax.dot_general(
                rows[at, :], weights[...], NN, preferred_element_type=F32
            )
        mats, keep = [], []
        for b in range(count):
            at = slice(b * BLOCK, (b + 1) * BLOCK)
            q = silu(proj[at, 0:HEAD])
            k = silu(proj[at, HEAD : 2 * HEAD])
            v = silu(proj[at, 2 * HEAD : 3 * HEAD])
            k = k * lax.rsqrt(jnp.sum(k * k, axis=1, keepdims=True) + 1e-06)
            small = proj[at, 3 * HEAD : 4 * HEAD]
            strength = largest * (1.0 / (1.0 + jnp.exp(-small[:, 0:1])))
            flipped = small.T
            x = flipped[0:8, :]
            soft = jnp.maximum(x, 0.0) + jnp.log1p(jnp.exp(-jnp.abs(x)))
            steps = extra_ref[pl.ds(start + b, 1), :] - speed * soft[1:2, :]
            cum_row = lax.dot_general(
                jnp.broadcast_to(steps, (8, BLOCK)), upper, NN, preferred_element_type=F32, precision=lax.Precision.HIGHEST
            )[0:1, :]
            across = jnp.broadcast_to(cum_row, (BLOCK, BLOCK))
            down = across.T
            total = jnp.broadcast_to(cum_row[:, BLOCK - 1 : BLOCK], (BLOCK, BLOCK))
            decay = jnp.exp(jnp.where(row >= col, down - across, -1e30))
            grow = jnp.exp(down)
            both = mm(jnp.concatenate([k, q], axis=0), k, NT)
            mats.append(jnp.where(row > col, both[:BLOCK] * decay * strength, 0.0))
            right = jnp.concatenate([v * strength, k * (grow * strength)], axis=1)
            keep.append((q * grow, both[BLOCK:] * decay, right, k * jnp.exp(total - down)))
            lasts[start + b] = jnp.exp(total[0:8, :])
        invs = invert_unit_lower(mats, row, col)
        for b in range(count):
            query_dec, scores, right, keys_dec = keep[b]
            solved = mm(invs[b], right)
            seen = mm(scores, solved)
            kept = mm(keys_dec, solved, TN)
            high[start + b, :, :HEAD] = kept[:, :HEAD]
            high[start + b, :, HEAD:] = seen[:, :HEAD]
            low[start + b, :HEAD, :] = (query_dec - seen[:, HEAD:]).astype(BF16)
            low[start + b, HEAD:, :] = kept[:, HEAD:].astype(BF16)
        return carry

    lax.fori_loop(0, 2, half, 0)
    maps = (row == col).astype(F32)
    memory = jnp.zeros((HEAD, HEAD), F32)
    for j in range(blocks):
        both = jnp.concatenate([maps, memory], axis=1).astype(BF16)
        out = mm(low[j], both)
        g_ref[j * BLOCK : (j + 1) * BLOCK, :] = out[:HEAD, :HEAD].astype(BF16)
        h_ref[j * BLOCK : (j + 1) * BLOCK, :] = out[:HEAD, HEAD:] + high[j, :, HEAD:]
        last = lasts[j, 0:1, :]
        maps = maps * last - out[HEAD:, :HEAD]
        memory = memory * last - out[HEAD:, HEAD:] + high[j, :, :HEAD]
    ab_ref[:, :HEAD] = maps.astype(BF16)
    ab_ref[:, HEAD:] = memory.astype(BF16)


def span_terms(scal, head, rows, query, key, value, strength, decay, extra):
    length, depth = rows.shape
    blocks = length // BLOCK
    width = 4 * HEAD
    chunks = 4
    smem = pl.BlockSpec(memory_space=pltpu.SMEM)
    vmem = pl.BlockSpec(memory_space=pltpu.VMEM)
    hbm = pl.BlockSpec(memory_space=pltpu.HBM)
    return pl.pallas_call(
        functools.partial(span_kernel, chunks),
        out_shape=(
            jax.ShapeDtypeStruct((length, HEAD), BF16),
            jax.ShapeDtypeStruct((length, HEAD), F32),
            jax.ShapeDtypeStruct((HEAD, 2 * HEAD), BF16),
        ),
        in_specs=[smem, smem, hbm, hbm, hbm, hbm, vmem, vmem, vmem],
        out_specs=(vmem, vmem, vmem),
        scratch_shapes=[
            pltpu.VMEM((length, depth), BF16),
            pltpu.VMEM((depth, width), BF16),
            pltpu.VMEM((length // 2, width), F32),
            pltpu.VMEM((blocks, 2 * HEAD, HEAD), BF16),
            pltpu.VMEM((blocks, HEAD, 2 * HEAD), F32),
            pltpu.VMEM((blocks, 8, HEAD), F32),
            pltpu.SemaphoreType.DMA((3 + chunks,)),
        ],
        compiler_params=pltpu.CompilerParams(vmem_limit_bytes=SPAN_LIMIT * 1024 * 1024),
        cost_estimate=pl.CostEstimate(
            flops=length * 2 * (depth * width + 40 * HEAD * HEAD * 4),
            bytes_accessed=2 * (rows.size + depth * width) + length * HEAD * 6,
            transcendentals=0,
        ),
    )(scal, head, *[pltpu.with_memory_space_constraint(x, pltpu.HBM) for x in (rows, query, key, value)], strength, decay, extra)


def row_kernel(here_ref, own_ref, one_ref, two_ref, three_ref, before_ref, total_ref, slots):
    here = here_ref[0]
    slots[here] = own_ref[...]
    slots[(here + 3) % 4] = one_ref[...]
    slots[(here + 2) % 4] = two_ref[...]
    slots[(here + 1) % 4] = three_ref[...]
    row = lax.broadcasted_iota(jnp.int32, (HEAD, 2 * HEAD), 0)
    col = lax.broadcasted_iota(jnp.int32, (HEAD, 2 * HEAD), 1)
    eye = (row == col).astype(F32)
    so_far = slots[0].astype(F32)
    before = jnp.where(here == 0, eye, so_far)
    for k in range(1, 4):
        piece = slots[k]
        own = jnp.where(col >= HEAD, piece.astype(F32), 0.0)
        so_far = mm(piece[:, :HEAD], so_far) + own
        if k < 3:
            before = jnp.where(here > k, so_far, before)
    before_ref[...] = before
    total_ref[...] = so_far.astype(BF16)


def compose_row(here, own, one, two, three):
    vmem = pl.BlockSpec(memory_space=pltpu.VMEM)
    return pl.pallas_call(
        row_kernel,
        out_shape=(jax.ShapeDtypeStruct((HEAD, 2 * HEAD), F32), jax.ShapeDtypeStruct((HEAD, 2 * HEAD), BF16)),
        in_specs=[pl.BlockSpec(memory_space=pltpu.SMEM)] + [vmem] * 4,
        out_specs=(vmem, vmem),
        scratch_shapes=[pltpu.VMEM((4, HEAD, 2 * HEAD), BF16)],
        compiler_params=pltpu.CompilerParams(vmem_limit_bytes=8 * 1024 * 1024),
        cost_estimate=pl.CostEstimate(flops=12 * HEAD**3, bytes_accessed=8 * HEAD * HEAD, transcendentals=0),
    )(here, own, one, two, three)


def apply_kernel(here_ref, one_ref, two_ref, three_ref, before_ref, g_ref, h_ref, gain_ref, out_ref, slots):
    here = here_ref[0]
    slots[(here + 3) % 4] = one_ref[...]
    slots[(here + 2) % 4] = two_ref[...]
    slots[(here + 1) % 4] = three_ref[...]
    memory = jnp.where(here > 0, slots[0][:, HEAD:].astype(F32), 0.0)
    for k in range(1, 3):
        piece = slots[k]
        moved = mm(piece[:, :HEAD], memory) + piece[:, HEAD:].astype(F32)
        memory = jnp.where(here > k, moved, memory)
    memory = mm(before_ref[:, :HEAD], memory) + before_ref[:, HEAD:]
    heads_out = mm(g_ref[...], memory) + h_ref[...]
    scale = lax.rsqrt(jnp.mean(heads_out * heads_out, axis=1, keepdims=True) + norm_eps)
    out_ref[...] = (heads_out * scale * gain_ref[...]).astype(BF16)


def apply_memory(here, one, two, three, before, g, h, gain):
    vmem = pl.BlockSpec(memory_space=pltpu.VMEM)
    return pl.pallas_call(
        apply_kernel,
        out_shape=jax.ShapeDtypeStruct(h.shape, BF16),
        in_specs=[pl.BlockSpec(memory_space=pltpu.SMEM)] + [vmem] * 7,
        out_specs=vmem,
        scratch_shapes=[pltpu.VMEM((4, HEAD, 2 * HEAD), BF16)],
        compiler_params=pltpu.CompilerParams(vmem_limit_bytes=8 * 1024 * 1024),
        cost_estimate=pl.CostEstimate(flops=h.size * 2 * HEAD, bytes_accessed=h.size * 8, transcendentals=0),
    )(here, one, two, three, before, g, h, gain.reshape(1, HEAD))


def output_kernel(x_ref, w_ref, out_ref, rows):
    @pl.when(pl.program_id(0) == 0)
    def _():
        for h in range(x_ref.shape[0]):
            rows[:, h * HEAD : (h + 1) * HEAD] = x_ref[h]

    out_ref[...] = mm(rows[...], w_ref[...]).astype(BF16)


def output_product(by_head, weights):
    depth, width = weights.shape
    count = by_head.shape[1]
    step = width // 8
    column = lambda i: (0, i)
    return pl.pallas_call(
        output_kernel,
        grid=(8,),
        out_shape=jax.ShapeDtypeStruct((count, width), BF16),
        in_specs=[pl.BlockSpec(by_head.shape, lambda i: (0, 0, 0)), pl.BlockSpec((depth, step), column)],
        out_specs=pl.BlockSpec((count, step), column),
        scratch_shapes=[pltpu.VMEM((count, depth), BF16)],
        cost_estimate=pl.CostEstimate(
            flops=2 * count * depth * width, bytes_accessed=2 * depth * width, transcendentals=0
        ),
        compiler_params=pltpu.CompilerParams(vmem_limit_bytes=32 * 1024 * 1024),
    )(by_head, pltpu.with_memory_space_constraint(weights, pltpu.HBM))


def route_columns(side, experts):
    tokens = side.shape[1]
    expert = lax.broadcasted_iota(jnp.int32, (experts, tokens), 0).astype(F32)
    first, second = side[0:1] == expert, side[1:2] == expert
    named = (first | second).astype(F32)
    row = lax.broadcasted_iota(jnp.int32, (tokens, tokens), 0)
    col = lax.broadcasted_iota(jnp.int32, (tokens, tokens), 1)
    earlier = ((row < col) & (row // TOKENS == col // TOKENS)).astype(F32)
    return first, named, mm(named, earlier)


def slot_rows(named, slots, e):
    tokens = named.shape[1]
    rows = tokens // TOKENS * SLOTS
    row = lax.broadcasted_iota(jnp.int32, (rows, tokens), 0)
    col = lax.broadcasted_iota(jnp.int32, (rows, tokens), 1)
    taken = jnp.where(named[e : e + 1] > 0.5, slots[e : e + 1], -1.0)
    return (taken == (row % SLOTS).astype(F32)) & (row // SLOTS == col // TOKENS)


def pack_kernel(experts, tok_ref, out_ref):
    width = out_ref.shape[1]
    side = tok_ref[:, width:].astype(F32).T
    _, named, slots = route_columns(side, experts)
    rows = out_ref.shape[0] // experts
    group = 4
    for e in range(0, experts, group):
        pick = jnp.concatenate([slot_rows(named, slots, e + i).astype(F32) for i in range(group)], axis=0)
        out_ref[e * rows : (e + group) * rows, :] = mm(pick, tok_ref[:, :width]).astype(BF16)


def pack_tokens(tokens, experts):
    count, width = tokens.shape
    vmem = pl.BlockSpec(memory_space=pltpu.VMEM)
    rows = count // TOKENS * SLOTS * experts
    return pl.pallas_call(
        functools.partial(pack_kernel, experts),
        out_shape=jax.ShapeDtypeStruct((rows, width - HEAD), BF16),
        in_specs=[vmem],
        out_specs=vmem,
        cost_estimate=pl.CostEstimate(flops=2 * rows * count * width, bytes_accessed=2 * rows * width, transcendentals=0),
    )(tokens)


def combine_kernel(experts, side_ref, back_ref, out_ref):
    side = side_ref[...].astype(F32).T
    first, named, slots = route_columns(side, experts)
    share = [side[2 + k : 3 + k] + side[4 + k : 5 + k] + side[6 + k : 7 + k] for k in range(2)]
    picks = []
    for e in range(experts):
        share_row = jnp.where(first[e : e + 1], share[0], share[1])
        picks.append(jnp.where(slot_rows(named, slots, e), share_row, 0.0))
    pick = jnp.concatenate(picks, axis=0)
    high = pick.astype(BF16)
    low = (pick - high.astype(F32)).astype(BF16)
    back = back_ref[...]
    out = mm(high, back, TN) + mm(low, back, TN)
    out_ref[...] = out.reshape(out_ref.shape).astype(BF16)


def combine_tokens(tokens, back, experts):
    count, _ = tokens.shape
    width = back.shape[1]
    shape = (count // TOKENS, TOKENS, width)
    return pl.pallas_call(
        functools.partial(combine_kernel, experts),
        grid=(1,),
        out_shape=jax.ShapeDtypeStruct(shape, BF16),
        in_specs=[
            pl.BlockSpec((count, HEAD), lambda i: (0, width // HEAD)),
            pl.BlockSpec(back.shape, lambda i: (0, 0)),
        ],
        out_specs=pl.BlockSpec(shape, lambda i: (0, 0, 0)),
        compiler_params=pltpu.CompilerParams(vmem_limit_bytes=24 * 1024 * 1024),
        cost_estimate=pl.CostEstimate(
            flops=4 * count * back.size, bytes_accessed=2 * back.size + 2 * count * width, transcendentals=0
        ),
    )(tokens, back)


def expert_kernel(own_ref, other_ref, gate_ref, up_ref, down_ref, mine_ref, theirs_ref, rows, gate, up, down, sems):
    half = own_ref.shape[0]
    pairs = (
        (own_ref, rows.at[pl.ds(0, half)]),
        (other_ref, rows.at[pl.ds(half, half)]),
        (gate_ref, gate),
        (up_ref, up),
        (down_ref, down),
    )
    copies = [pltpu.make_async_copy(src, dst, sems.at[i]) for i, (src, dst) in enumerate(pairs)]
    for copy in copies:
        copy.start()
    for copy in copies[:3]:
        copy.wait()
    gated = silu(mm(rows[...], gate[...], NT))
    copies[3].wait()
    hidden = (gated * mm(rows[...], up[...], NT)).astype(BF16)
    copies[4].wait()
    theirs_ref[...] = mm(hidden[half:], down[...]).astype(BF16)
    mine_ref[...] = mm(hidden[:half], down[...]).astype(BF16)


def expert_sums(own, other, gate, up, down):
    half, width = own.shape
    units = gate.shape[0]
    out = jax.ShapeDtypeStruct((half, width), BF16)
    vmem = pl.BlockSpec(memory_space=pltpu.VMEM)
    return pl.pallas_call(
        expert_kernel,
        out_shape=(out, out),
        in_specs=[pl.BlockSpec(memory_space=pl.ANY)] * 5,
        out_specs=(vmem, vmem),
        scratch_shapes=[
            pltpu.VMEM((2 * half, width), BF16),
            pltpu.VMEM((units, width), BF16),
            pltpu.VMEM((units, width), BF16),
            pltpu.VMEM((units, width), BF16),
            pltpu.SemaphoreType.DMA((5,)),
        ],
        cost_estimate=pl.CostEstimate(
            flops=12 * half * width * units, bytes_accessed=6 * units * width + 8 * half * width, transcendentals=0
        ),
        compiler_params=pltpu.CompilerParams(vmem_limit_bytes=36 * 1024 * 1024),
    )(own, other, *[pltpu.with_memory_space_constraint(x, pltpu.HBM) for x in (gate, up, down)])


def around(x, axis):
    size = lax.axis_size(axis)
    out = []
    for k in range(1, size):
        out.append(lax.ppermute(x, axis, [(i, (i + k) % size) for i in range(size)]))
    return out


def mixed_step(
    mixer_input_rows,
    mixer_norm_gain,
    query_weight,
    key_weight,
    value_weight,
    write_strength_projection,
    decay_projection,
    head_decay_speed,
    largest_write_strength,
    extra_log_decay,
    head_norm_gain,
    mixer_output_weight,
    expert_input_rows,
    expert_norm_gain,
    routes,
    expert_route_weight,
    gate_weight,
    up_weight,
    down_weight,
):
    head = lax.axis_index(TP)
    experts = gate_weight.shape[0] * lax.axis_size(EP)
    cross = lambda x: lax.ppermute(x, "tp_1", [(0, 1), (1, 0)])

    mix_normed = rms_scale(mixer_input_rows, mixer_norm_gain)
    exp_normed = rms_scale(expert_input_rows, expert_norm_gain)
    parts, rest = [], expert_route_weight
    for _ in range(3):
        part = lax.reduce_precision(rest, 8, 7)
        parts.append(part.astype(BF16))
        rest = rest - part
    side = jnp.concatenate([routes.astype(BF16)] + parts, axis=1)
    side = jnp.pad(side, ((0, 0), (0, HEAD - side.shape[1])))
    tokens = lax.all_gather(jnp.concatenate([exp_normed, side], axis=1), "tp_0", axis=0, tiled=True)
    tokens, mix_normed = lax.optimization_barrier((tokens, mix_normed))
    mix_rows = lax.all_gather(mix_normed, TP, axis=0, tiled=True)
    packed = pack_tokens(tokens, experts)
    exp_rows = lax.all_to_all(packed, EP, split_axis=0, concat_axis=0, tiled=True)
    other_rows = cross(exp_rows)
    mine, theirs = expert_sums(exp_rows, other_rows, gate_weight[0].T, up_weight[0].T, down_weight[0])
    pair = (mine.astype(F32) + cross(theirs).astype(F32)).astype(BF16)
    back = lax.all_to_all(pair, EP, split_axis=0, concat_axis=0, tiled=True)
    combined = combine_tokens(tokens, back, experts)

    scal = jnp.concatenate([head_decay_speed, largest_write_strength])
    extra = extra_log_decay.reshape(-1, BLOCK)
    gains, local, span = span_terms(
        scal,
        head[None],
        mix_rows,
        query_weight,
        key_weight,
        value_weight,
        write_strength_projection.T,
        decay_projection.T,
        extra,
    )
    row_pieces = around(span, "ep_1")
    before, total = compose_row(lax.axis_index("ep_1")[None], span, *row_pieces)
    mixed = apply_memory(lax.axis_index("ep_0")[None], *around(total, "ep_0"), before, gains, local, head_norm_gain)

    by_head = lax.all_to_all(mixed.reshape(-1, BLOCK, HEAD), TP, split_axis=0, concat_axis=0, tiled=True)
    w_whole = lax.all_gather(mixer_output_weight, TP, axis=0, tiled=True)
    mix_out = output_product(by_head, w_whole)

    pieces = lax.all_to_all(combined, "tp_0", split_axis=0, concat_axis=0, tiled=True)
    exp_out = jnp.sum(pieces.astype(F32), axis=0).astype(BF16)
    return (mix_out, exp_out)


def solution(mesh):
    torus = Mesh(mesh.devices.reshape(4, 4, 8, 2), ("ep_0", "ep_1", "tp_0", "tp_1"))
    placed = (
        P(EP_TP, None),
        P(),
        P(None, TP),
        P(None, TP),
        P(None, TP),
        P(),
        P(),
        P(TP),
        P(TP),
        P(EP, TP),
        P(),
        P(TP, None),
        P(EP_TP, None),
        P(),
        P(EP_TP, None),
        P(EP_TP, None),
        P(EP, None, TP),
        P(EP, None, TP),
        P(EP, TP, None),
    )
    return jax.shard_map(
        mixed_step,
        mesh=torus,
        in_specs=placed,
        out_specs=(P(EP_TP, None), P(EP_TP, None)),
        check_vma=False,
    )
```

```python
import functools

import jax
import jax.numpy as jnp
from jax import lax
from jax.experimental import pallas as pl
from jax.experimental.pallas import tpu as pltpu
from jax.sharding import Mesh
from jax.sharding import PartitionSpec as P


HEAD = 128
BLOCK = 128
TOKENS = 8
SLOTS = 2
SPAN_LIMIT = 44
EP = ("ep_0", "ep_1")
TP = ("tp_0", "tp_1")
EP_TP = ("ep_0", "ep_1", "tp_0", "tp_1")
F32 = jnp.float32
BF16 = jnp.bfloat16


norm_eps = 1e-06
NN = (((1,), (0,)), ((), ()))
NT = (((1,), (1,)), ((), ()))
TN = (((0,), (0,)), ((), ()))


def mm(a, b, dims=NN):
    return lax.dot_general(a.astype(BF16), b.astype(BF16), dims, preferred_element_type=F32)


def silu(x):
    return x / (1.0 + jnp.exp(-x))


def rms_scale(rows_in, gain_vec):
    widened = rows_in.astype(F32)
    scaled = widened * lax.rsqrt(jnp.mean(widened * widened, axis=-1, keepdims=True) + norm_eps)
    return (scaled * gain_vec).astype(BF16)


def invert_unit_lower(mats, row, col):
    apart = row ^ col
    eye = (row == col).astype(F32)
    size = 1
    invs = None
    while size < BLOCK:
        pick = (apart >= size) & (apart < 2 * size)
        parts = [jnp.where(pick, m, 0.0) for m in mats]
        if invs is None:
            invs = [eye - p for p in parts]
        else:
            invs_low = [x.astype(BF16) for x in invs]
            half = [mm(p, x) for p, x in zip(parts, invs_low)]
            invs = [x - mm(xl, h) for x, xl, h in zip(invs, invs_low, half)]
        size *= 2
    return invs


def span_kernel(
    chunks, scal_ref, head_ref, rows_ref, q_ref, k_ref, v_ref, strength_ref, decay_ref, extra_ref,
    g_ref, h_ref, ab_ref, rows, weights, proj, low, high, lasts, sems
):
    tall = rows_ref.shape[0] // chunks
    blocks = rows_ref.shape[0] // BLOCK
    count = blocks // 2
    copies = [
        pltpu.make_async_copy(ref, weights.at[:, pl.ds(i * HEAD, HEAD)], sems.at[i])
        for i, ref in enumerate((q_ref, k_ref, v_ref))
    ]
    row_copies = [
        pltpu.make_async_copy(rows_ref.at[pl.ds(i * tall, tall)], rows.at[pl.ds(i * tall, tall)], sems.at[3 + i])
        for i in range(chunks)
    ]
    for copy in copies + row_copies:
        copy.start()
    heads = strength_ref.shape[0]
    pick_row = lax.broadcasted_iota(jnp.int32, (heads, HEAD), 0) == head_ref[0]
    pick_col = lax.broadcasted_iota(jnp.int32, (heads, HEAD), 1)
    weights[:, 3 * HEAD :] = (
        mm(strength_ref[...], (pick_row & (pick_col == 0)).astype(BF16), TN)
        + mm(decay_ref[...], (pick_row & (pick_col == 1)).astype(BF16), TN)
    ).astype(BF16)
    row = lax.broadcasted_iota(jnp.int32, (BLOCK, BLOCK), 0)
    col = lax.broadcasted_iota(jnp.int32, (BLOCK, BLOCK), 1)
    upper = (row <= col).astype(F32)
    speed, largest = scal_ref[0], scal_ref[1]
    for copy in copies:
        copy.wait()

    def half(i, carry):
        start = i * count
        for c in range(chunks // 2):
            chunk = i * (chunks // 2) + c
            at = pl.ds(pl.multiple_of(chunk * tall, tall), tall)
            pltpu.make_async_copy(rows_ref.at[at], rows.at[at], sems.at[3 + chunk]).wait()
            proj[c * tall : (c + 1) * tall, :] = lax.dot_general(
                rows[at, :], weights[...], NN, preferred_element_type=F32
            )
        mats, keep = [], []
        for b in range(count):
            at = slice(b * BLOCK, (b + 1) * BLOCK)
            q = silu(proj[at, 0:HEAD])
            k = silu(proj[at, HEAD : 2 * HEAD])
            v = silu(proj[at, 2 * HEAD : 3 * HEAD])
            k = k * lax.rsqrt(jnp.sum(k * k, axis=1, keepdims=True) + 1e-06)
            small = proj[at, 3 * HEAD : 4 * HEAD]
            strength = largest * (1.0 / (1.0 + jnp.exp(-small[:, 0:1])))
            flipped = small.T
            x = flipped[0:8, :]
            soft = jnp.maximum(x, 0.0) + jnp.log1p(jnp.exp(-jnp.abs(x)))
            steps = extra_ref[pl.ds(start + b, 1), :] - speed * soft[1:2, :]
            cum_row = lax.dot_general(
                jnp.broadcast_to(steps, (8, BLOCK)), upper, NN, preferred_element_type=F32, precision=lax.Precision.HIGHEST
            )[0:1, :]
            across = jnp.broadcast_to(cum_row, (BLOCK, BLOCK))
            down = across.T
            total = jnp.broadcast_to(cum_row[:, BLOCK - 1 : BLOCK], (BLOCK, BLOCK))
            decay = jnp.exp(jnp.where(row >= col, down - across, -1e30))
            grow = jnp.exp(down)
            both = mm(jnp.concatenate([k, q], axis=0), k, NT)
            mats.append(jnp.where(row > col, both[:BLOCK] * decay * strength, 0.0))
            right = jnp.concatenate([v * strength, k * (grow * strength)], axis=1)
            keep.append((q * grow, both[BLOCK:] * decay, right, k * jnp.exp(total - down)))
            lasts[start + b] = jnp.exp(total[0:8, :])
        invs = invert_unit_lower(mats, row, col)
        for b in range(count):
            query_dec, scores, right, keys_dec = keep[b]
            solved = mm(invs[b], right)
            seen = mm(scores, solved)
            kept = mm(keys_dec, solved, TN)
            high[start + b, :, :HEAD] = kept[:, :HEAD]
            high[start + b, :, HEAD:] = seen[:, :HEAD]
            low[start + b, :HEAD, :] = (query_dec - seen[:, HEAD:]).astype(BF16)
            low[start + b, HEAD:, :] = kept[:, HEAD:].astype(BF16)
        return carry

    lax.fori_loop(0, 2, half, 0)
    maps = (row == col).astype(F32)
    memory = jnp.zeros((HEAD, HEAD), F32)
    for j in range(blocks):
        both = jnp.concatenate([maps, memory], axis=1).astype(BF16)
        out = mm(low[j], both)
        g_ref[j * BLOCK : (j + 1) * BLOCK, :] = out[:HEAD, :HEAD].astype(BF16)
        h_ref[j * BLOCK : (j + 1) * BLOCK, :] = out[:HEAD, HEAD:] + high[j, :, HEAD:]
        last = lasts[j, 0:1, :]
        maps = maps * last - out[HEAD:, :HEAD]
        memory = memory * last - out[HEAD:, HEAD:] + high[j, :, :HEAD]
    ab_ref[:, :HEAD] = maps.astype(BF16)
    ab_ref[:, HEAD:] = memory.astype(BF16)


def span_terms(scal, head, rows, query, key, value, strength, decay, extra):
    length, depth = rows.shape
    blocks = length // BLOCK
    width = 4 * HEAD
    chunks = 4
    smem = pl.BlockSpec(memory_space=pltpu.SMEM)
    vmem = pl.BlockSpec(memory_space=pltpu.VMEM)
    hbm = pl.BlockSpec(memory_space=pltpu.HBM)
    return pl.pallas_call(
        functools.partial(span_kernel, chunks),
        out_shape=(
            jax.ShapeDtypeStruct((length, HEAD), BF16),
            jax.ShapeDtypeStruct((length, HEAD), F32),
            jax.ShapeDtypeStruct((HEAD, 2 * HEAD), BF16),
        ),
        in_specs=[smem, smem, hbm, hbm, hbm, hbm, vmem, vmem, vmem],
        out_specs=(vmem, vmem, vmem),
        scratch_shapes=[
            pltpu.VMEM((length, depth), BF16),
            pltpu.VMEM((depth, width), BF16),
            pltpu.VMEM((length // 2, width), F32),
            pltpu.VMEM((blocks, 2 * HEAD, HEAD), BF16),
            pltpu.VMEM((blocks, HEAD, 2 * HEAD), F32),
            pltpu.VMEM((blocks, 8, HEAD), F32),
            pltpu.SemaphoreType.DMA((3 + chunks,)),
        ],
        compiler_params=pltpu.CompilerParams(vmem_limit_bytes=SPAN_LIMIT * 1024 * 1024),
        cost_estimate=pl.CostEstimate(
            flops=length * 2 * (depth * width + 40 * HEAD * HEAD * 4),
            bytes_accessed=2 * (rows.size + depth * width) + length * HEAD * 6,
            transcendentals=0,
        ),
    )(scal, head, *[pltpu.with_memory_space_constraint(x, pltpu.HBM) for x in (rows, query, key, value)], strength, decay, extra)


def row_kernel(here_ref, own_ref, one_ref, two_ref, three_ref, before_ref, total_ref, slots):
    here = here_ref[0]
    slots[here] = own_ref[...]
    slots[(here + 3) % 4] = one_ref[...]
    slots[(here + 2) % 4] = two_ref[...]
    slots[(here + 1) % 4] = three_ref[...]
    row = lax.broadcasted_iota(jnp.int32, (HEAD, 2 * HEAD), 0)
    col = lax.broadcasted_iota(jnp.int32, (HEAD, 2 * HEAD), 1)
    eye = (row == col).astype(F32)
    so_far = slots[0].astype(F32)
    before = jnp.where(here == 0, eye, so_far)
    for k in range(1, 4):
        piece = slots[k]
        own = jnp.where(col >= HEAD, piece.astype(F32), 0.0)
        so_far = mm(piece[:, :HEAD], so_far) + own
        if k < 3:
            before = jnp.where(here > k, so_far, before)
    before_ref[...] = before
    total_ref[...] = so_far.astype(BF16)


def compose_row(here, own, one, two, three):
    vmem = pl.BlockSpec(memory_space=pltpu.VMEM)
    return pl.pallas_call(
        row_kernel,
        out_shape=(jax.ShapeDtypeStruct((HEAD, 2 * HEAD), F32), jax.ShapeDtypeStruct((HEAD, 2 * HEAD), BF16)),
        in_specs=[pl.BlockSpec(memory_space=pltpu.SMEM)] + [vmem] * 4,
        out_specs=(vmem, vmem),
        scratch_shapes=[pltpu.VMEM((4, HEAD, 2 * HEAD), BF16)],
        compiler_params=pltpu.CompilerParams(vmem_limit_bytes=8 * 1024 * 1024),
        cost_estimate=pl.CostEstimate(flops=12 * HEAD**3, bytes_accessed=8 * HEAD * HEAD, transcendentals=0),
    )(here, own, one, two, three)


def apply_kernel(here_ref, one_ref, two_ref, three_ref, before_ref, g_ref, h_ref, gain_ref, out_ref, slots):
    here = here_ref[0]
    slots[(here + 3) % 4] = one_ref[...]
    slots[(here + 2) % 4] = two_ref[...]
    slots[(here + 1) % 4] = three_ref[...]
    memory = jnp.where(here > 0, slots[0][:, HEAD:].astype(F32), 0.0)
    for k in range(1, 3):
        piece = slots[k]
        moved = mm(piece[:, :HEAD], memory) + piece[:, HEAD:].astype(F32)
        memory = jnp.where(here > k, moved, memory)
    memory = mm(before_ref[:, :HEAD], memory) + before_ref[:, HEAD:]
    heads_out = mm(g_ref[...], memory) + h_ref[...]
    scale = lax.rsqrt(jnp.mean(heads_out * heads_out, axis=1, keepdims=True) + norm_eps)
    out_ref[...] = (heads_out * scale * gain_ref[...]).astype(BF16)


def apply_memory(here, one, two, three, before, g, h, gain):
    vmem = pl.BlockSpec(memory_space=pltpu.VMEM)
    return pl.pallas_call(
        apply_kernel,
        out_shape=jax.ShapeDtypeStruct(h.shape, BF16),
        in_specs=[pl.BlockSpec(memory_space=pltpu.SMEM)] + [vmem] * 7,
        out_specs=vmem,
        scratch_shapes=[pltpu.VMEM((4, HEAD, 2 * HEAD), BF16)],
        compiler_params=pltpu.CompilerParams(vmem_limit_bytes=8 * 1024 * 1024),
        cost_estimate=pl.CostEstimate(flops=h.size * 2 * HEAD, bytes_accessed=h.size * 8, transcendentals=0),
    )(here, one, two, three, before, g, h, gain.reshape(1, HEAD))


def sum_kernel(*refs):
    total = refs[0][...].astype(F32)
    for ref in refs[1:-1]:
        total = total + ref[...].astype(F32)
    refs[-1][...] = total.astype(BF16)


def sum_parts(parts):
    vmem = pl.BlockSpec(memory_space=pltpu.VMEM)
    return pl.pallas_call(
        sum_kernel,
        out_shape=jax.ShapeDtypeStruct(parts[0].shape, BF16),
        in_specs=[vmem] * len(parts),
        out_specs=vmem,
        compiler_params=pltpu.CompilerParams(vmem_limit_bytes=4 * 1024 * 1024),
        cost_estimate=pl.CostEstimate(flops=10**6, bytes_accessed=2 * 9 * parts[0].size, transcendentals=0),
    )(*parts)


def output_kernel(chunks, x_ref, w_ref, out_ref, weights, total, sems):
    tall = w_ref.shape[0] // chunks
    copies = [
        pltpu.make_async_copy(w_ref.at[pl.ds(i * tall, tall)], weights.at[pl.ds(i * tall, tall)], sems.at[i])
        for i in range(chunks)
    ]
    for copy in copies:
        copy.start()
    heads = tall // HEAD
    for i, copy in enumerate(copies):
        rows = jnp.concatenate([x_ref[i * heads + h] for h in range(heads)], axis=1)
        copy.wait()
        part = mm(rows, weights[i * tall : (i + 1) * tall, :])
        if i == 0:
            total[...] = part
        elif i < chunks - 1:
            total[...] += part
        else:
            out_ref[...] = (total[...] + part).astype(BF16)


def output_product(by_head, weights):
    depth, width = weights.shape
    count = by_head.shape[1]
    chunks = 4
    vmem = pl.BlockSpec(memory_space=pltpu.VMEM)
    return pl.pallas_call(
        functools.partial(output_kernel, chunks),
        out_shape=jax.ShapeDtypeStruct((count, width), BF16),
        in_specs=[vmem, pl.BlockSpec(memory_space=pltpu.HBM)],
        out_specs=vmem,
        scratch_shapes=[
            pltpu.VMEM((depth, width), BF16),
            pltpu.VMEM((count, width), F32),
            pltpu.SemaphoreType.DMA((chunks,)),
        ],
        cost_estimate=pl.CostEstimate(
            flops=2 * count * depth * width, bytes_accessed=2 * depth * width, transcendentals=0
        ),
        compiler_params=pltpu.CompilerParams(vmem_limit_bytes=32 * 1024 * 1024),
    )(by_head, pltpu.with_memory_space_constraint(weights, pltpu.HBM))


def route_columns(side, experts):
    tokens = side.shape[1]
    expert = lax.broadcasted_iota(jnp.int32, (experts, tokens), 0).astype(F32)
    first, second = side[0:1] == expert, side[1:2] == expert
    named = (first | second).astype(F32)
    row = lax.broadcasted_iota(jnp.int32, (tokens, tokens), 0)
    col = lax.broadcasted_iota(jnp.int32, (tokens, tokens), 1)
    earlier = ((row < col) & (row // TOKENS == col // TOKENS)).astype(F32)
    return first, named, mm(named, earlier)


def slot_rows(named, slots, e):
    tokens = named.shape[1]
    rows = tokens // TOKENS * SLOTS
    row = lax.broadcasted_iota(jnp.int32, (rows, tokens), 0)
    col = lax.broadcasted_iota(jnp.int32, (rows, tokens), 1)
    taken = jnp.where(named[e : e + 1] > 0.5, slots[e : e + 1], -1.0)
    return (taken == (row % SLOTS).astype(F32)) & (row // SLOTS == col // TOKENS)


def pack_kernel(experts, tok_ref, out_ref):
    width = out_ref.shape[1]
    side = tok_ref[:, width:].astype(F32).T
    _, named, slots = route_columns(side, experts)
    rows = out_ref.shape[0] // experts
    group = 4
    for e in range(0, experts, group):
        pick = jnp.concatenate([slot_rows(named, slots, e + i).astype(F32) for i in range(group)], axis=0)
        out_ref[e * rows : (e + group) * rows, :] = mm(pick, tok_ref[:, :width]).astype(BF16)


def pack_tokens(tokens, experts):
    count, width = tokens.shape
    vmem = pl.BlockSpec(memory_space=pltpu.VMEM)
    rows = count // TOKENS * SLOTS * experts
    return pl.pallas_call(
        functools.partial(pack_kernel, experts),
        out_shape=jax.ShapeDtypeStruct((rows, width - HEAD), BF16),
        in_specs=[vmem],
        out_specs=vmem,
        cost_estimate=pl.CostEstimate(flops=2 * rows * count * width, bytes_accessed=2 * rows * width, transcendentals=0),
    )(tokens)


def combine_kernel(experts, devices, here_ref, side_ref, back_ref, *refs):
    out_refs, total = refs[:devices], refs[devices]
    side = side_ref[...].astype(F32).T
    first, named, slots = route_columns(side, experts)
    share = [side[2 + k : 3 + k] + side[4 + k : 5 + k] + side[6 + k : 7 + k] for k in range(2)]
    picks = []
    for e in range(experts):
        share_row = jnp.where(first[e : e + 1], share[0], share[1])
        picks.append(jnp.where(slot_rows(named, slots, e), share_row, 0.0))
    pick = jnp.concatenate(picks, axis=0)
    high = pick.astype(BF16)
    low = (pick - high.astype(F32)).astype(BF16)
    back = back_ref[...]
    total[...] = (mm(high, back, TN) + mm(low, back, TN)).reshape(total.shape)
    for k, out_ref in enumerate(out_refs):
        out_ref[...] = total[(here_ref[0] + k) % len(out_refs)].astype(BF16)


def combine_tokens(here, tokens, back, experts):
    count, _ = tokens.shape
    width = back.shape[1]
    devices = count // TOKENS
    piece = (TOKENS, width)
    return pl.pallas_call(
        functools.partial(combine_kernel, experts, devices),
        grid=(1,),
        out_shape=[jax.ShapeDtypeStruct(piece, BF16)] * devices,
        in_specs=[
            pl.BlockSpec(memory_space=pltpu.SMEM),
            pl.BlockSpec((count, HEAD), lambda i: (0, width // HEAD)),
            pl.BlockSpec(back.shape, lambda i: (0, 0)),
        ],
        out_specs=[pl.BlockSpec(piece, lambda i: (0, 0))] * devices,
        scratch_shapes=[pltpu.VMEM((devices, *piece), F32)],
        compiler_params=pltpu.CompilerParams(vmem_limit_bytes=24 * 1024 * 1024),
        cost_estimate=pl.CostEstimate(
            flops=4 * count * back.size, bytes_accessed=2 * back.size + 2 * count * width, transcendentals=0
        ),
    )(here, tokens, back)


def expert_kernel(own_ref, other_ref, gate_ref, up_ref, down_ref, mine_ref, theirs_ref, rows, gate, up, down, sems):
    half = own_ref.shape[0]
    pairs = (
        (own_ref, rows.at[pl.ds(0, half)]),
        (other_ref, rows.at[pl.ds(half, half)]),
        (gate_ref, gate),
        (up_ref, up),
        (down_ref, down),
    )
    copies = [pltpu.make_async_copy(src, dst, sems.at[i]) for i, (src, dst) in enumerate(pairs)]
    for copy in copies:
        copy.start()
    for copy in copies[:3]:
        copy.wait()
    gated = silu(mm(rows[...], gate[...], NT))
    copies[3].wait()
    hidden = (gated * mm(rows[...], up[...], NT)).astype(BF16)
    copies[4].wait()
    theirs_ref[...] = mm(hidden[half:], down[...]).astype(BF16)
    mine_ref[...] = mm(hidden[:half], down[...]).astype(BF16)


def expert_sums(own, other, gate, up, down):
    half, width = own.shape
    units = gate.shape[0]
    out = jax.ShapeDtypeStruct((half, width), BF16)
    vmem = pl.BlockSpec(memory_space=pltpu.VMEM)
    return pl.pallas_call(
        expert_kernel,
        out_shape=(out, out),
        in_specs=[pl.BlockSpec(memory_space=pl.ANY)] * 5,
        out_specs=(vmem, vmem),
        scratch_shapes=[
            pltpu.VMEM((2 * half, width), BF16),
            pltpu.VMEM((units, width), BF16),
            pltpu.VMEM((units, width), BF16),
            pltpu.VMEM((units, width), BF16),
            pltpu.SemaphoreType.DMA((5,)),
        ],
        cost_estimate=pl.CostEstimate(
            flops=12 * half * width * units, bytes_accessed=6 * units * width + 8 * half * width, transcendentals=0
        ),
        compiler_params=pltpu.CompilerParams(vmem_limit_bytes=36 * 1024 * 1024),
    )(own, other, *[pltpu.with_memory_space_constraint(x, pltpu.HBM) for x in (gate, up, down)])


def around(x, axis):
    size = lax.axis_size(axis)
    out = []
    for k in range(1, size):
        out.append(lax.ppermute(x, axis, [(i, (i + k) % size) for i in range(size)]))
    return out


def mixed_step(
    mixer_input_rows,
    mixer_norm_gain,
    query_weight,
    key_weight,
    value_weight,
    write_strength_projection,
    decay_projection,
    head_decay_speed,
    largest_write_strength,
    extra_log_decay,
    head_norm_gain,
    mixer_output_weight,
    expert_input_rows,
    expert_norm_gain,
    routes,
    expert_route_weight,
    gate_weight,
    up_weight,
    down_weight,
):
    head = lax.axis_index(TP)
    experts = gate_weight.shape[0] * lax.axis_size(EP)
    cross = lambda x: lax.ppermute(x, "tp_1", [(0, 1), (1, 0)])

    mix_normed = rms_scale(mixer_input_rows, mixer_norm_gain)
    mix_rows = lax.all_gather(mix_normed, TP, axis=0, tiled=True)

    exp_normed = rms_scale(expert_input_rows, expert_norm_gain)
    parts, rest = [], expert_route_weight
    for _ in range(3):
        part = lax.reduce_precision(rest, 8, 7)
        parts.append(part.astype(BF16))
        rest = rest - part
    side = jnp.concatenate([routes.astype(BF16)] + parts, axis=1)
    side = jnp.pad(side, ((0, 0), (0, HEAD - side.shape[1])))
    own = jnp.concatenate([exp_normed, side], axis=1)
    copies = jnp.broadcast_to(own, (lax.axis_size("tp_0"), *own.shape))
    tokens = lax.all_to_all(copies, "tp_0", split_axis=0, concat_axis=0, tiled=True).reshape(-1, own.shape[1])
    packed = pack_tokens(tokens, experts)
    exp_rows = lax.all_to_all(packed, EP, split_axis=0, concat_axis=0, tiled=True)
    other_rows = cross(exp_rows)
    mine, theirs = expert_sums(exp_rows, other_rows, gate_weight[0].T, up_weight[0].T, down_weight[0])
    pair = (mine.astype(F32) + cross(theirs).astype(F32)).astype(BF16)
    back = lax.all_to_all(pair, EP, split_axis=0, concat_axis=0, tiled=True)
    parts = combine_tokens(lax.axis_index("tp_0")[None], tokens, back, experts)

    scal = jnp.concatenate([head_decay_speed, largest_write_strength])
    extra = extra_log_decay.reshape(-1, BLOCK)
    gains, local, span = span_terms(
        scal,
        head[None],
        mix_rows,
        query_weight,
        key_weight,
        value_weight,
        write_strength_projection.T,
        decay_projection.T,
        extra,
    )
    row_pieces = around(span, "ep_1")
    before, total = compose_row(lax.axis_index("ep_1")[None], span, *row_pieces)
    mixed = apply_memory(lax.axis_index("ep_0")[None], *around(total, "ep_0"), before, gains, local, head_norm_gain)

    by_head = lax.all_to_all(mixed.reshape(-1, BLOCK, HEAD), TP, split_axis=0, concat_axis=0, tiled=True)
    w_whole = lax.all_gather(mixer_output_weight, TP, axis=0, tiled=True)
    mix_out = output_product(by_head, w_whole)

    ring = lax.axis_size("tp_0")
    arrived = [parts[0]]
    for k in range(1, ring):
        arrived.append(lax.ppermute(parts[k], "tp_0", [(i, (i + k) % ring) for i in range(ring)]))
    exp_out = sum_parts(arrived)
    return (mix_out, exp_out)


def solution(mesh):
    torus = Mesh(mesh.devices.reshape(4, 4, 8, 2), ("ep_0", "ep_1", "tp_0", "tp_1"))
    placed = (
        P(EP_TP, None),
        P(),
        P(None, TP),
        P(None, TP),
        P(None, TP),
        P(),
        P(),
        P(TP),
        P(TP),
        P(EP, TP),
        P(),
        P(TP, None),
        P(EP_TP, None),
        P(),
        P(EP_TP, None),
        P(EP_TP, None),
        P(EP, None, TP),
        P(EP, None, TP),
        P(EP, TP, None),
    )
    return jax.shard_map(
        mixed_step,
        mesh=torus,
        in_specs=placed,
        out_specs=(P(EP_TP, None), P(EP_TP, None)),
        check_vma=False,
    )
```

```python
import functools

import jax
import jax.numpy as jnp
from jax import lax
from jax.experimental import pallas as pl
from jax.experimental.pallas import tpu as pltpu
from jax.sharding import Mesh
from jax.sharding import PartitionSpec as P


HEAD = 128
BLOCK = 128
TOKENS = 8
SLOTS = 2
SPAN_LIMIT = 44
EP = ("ep_0", "ep_1")
TP = ("tp_0", "tp_1")
EP_TP = ("ep_0", "ep_1", "tp_0", "tp_1")
F32 = jnp.float32
BF16 = jnp.bfloat16


norm_eps = 1e-06
NN = (((1,), (0,)), ((), ()))
NT = (((1,), (1,)), ((), ()))
TN = (((0,), (0,)), ((), ()))


def mm(a, b, dims=NN):
    return lax.dot_general(a.astype(BF16), b.astype(BF16), dims, preferred_element_type=F32)


def silu(x):
    return x / (1.0 + jnp.exp(-x))


def rms_scale(rows_in, gain_vec):
    widened = rows_in.astype(F32)
    scaled = widened * lax.rsqrt(jnp.mean(widened * widened, axis=-1, keepdims=True) + norm_eps)
    return (scaled * gain_vec).astype(BF16)


def invert_unit_lower(mats, row, col):
    apart = row ^ col
    eye = (row == col).astype(F32)
    size = 1
    invs = None
    while size < BLOCK:
        pick = (apart >= size) & (apart < 2 * size)
        parts = [jnp.where(pick, m, 0.0) for m in mats]
        if invs is None:
            invs = [eye - p for p in parts]
        else:
            invs_low = [x.astype(BF16) for x in invs]
            half = [mm(p, x) for p, x in zip(parts, invs_low)]
            invs = [x - mm(xl, h) for x, xl, h in zip(invs, invs_low, half)]
        size *= 2
    return invs


def span_kernel(
    chunks, scal_ref, head_ref, rows_ref, q_ref, k_ref, v_ref, strength_ref, decay_ref, extra_ref,
    g_ref, h_ref, ab_ref, rows, weights, proj, low, high, lasts, sems
):
    tall = rows_ref.shape[0] // chunks
    blocks = rows_ref.shape[0] // BLOCK
    count = blocks // 2
    copies = [
        pltpu.make_async_copy(ref, weights.at[:, pl.ds(i * HEAD, HEAD)], sems.at[i])
        for i, ref in enumerate((q_ref, k_ref, v_ref))
    ]
    row_copies = [
        pltpu.make_async_copy(rows_ref.at[pl.ds(i * tall, tall)], rows.at[pl.ds(i * tall, tall)], sems.at[3 + i])
        for i in range(chunks)
    ]
    for copy in copies + row_copies:
        copy.start()
    heads = strength_ref.shape[0]
    pick_row = lax.broadcasted_iota(jnp.int32, (heads, HEAD), 0) == head_ref[0]
    pick_col = lax.broadcasted_iota(jnp.int32, (heads, HEAD), 1)
    weights[:, 3 * HEAD :] = (
        mm(strength_ref[...], (pick_row & (pick_col == 0)).astype(BF16), TN)
        + mm(decay_ref[...], (pick_row & (pick_col == 1)).astype(BF16), TN)
    ).astype(BF16)
    row = lax.broadcasted_iota(jnp.int32, (BLOCK, BLOCK), 0)
    col = lax.broadcasted_iota(jnp.int32, (BLOCK, BLOCK), 1)
    upper = (row <= col).astype(F32)
    speed, largest = scal_ref[0], scal_ref[1]
    for copy in copies:
        copy.wait()

    def half(i, carry):
        start = i * count
        for c in range(chunks // 2):
            chunk = i * (chunks // 2) + c
            at = pl.ds(pl.multiple_of(chunk * tall, tall), tall)
            pltpu.make_async_copy(rows_ref.at[at], rows.at[at], sems.at[3 + chunk]).wait()
            proj[c * tall : (c + 1) * tall, :] = lax.dot_general(
                rows[at, :], weights[...], NN, preferred_element_type=F32
            )
        mats, keep = [], []
        for b in range(count):
            at = slice(b * BLOCK, (b + 1) * BLOCK)
            q = silu(proj[at, 0:HEAD])
            k = silu(proj[at, HEAD : 2 * HEAD])
            v = silu(proj[at, 2 * HEAD : 3 * HEAD])
            k = k * lax.rsqrt(jnp.sum(k * k, axis=1, keepdims=True) + 1e-06)
            small = proj[at, 3 * HEAD : 4 * HEAD]
            strength = largest * (1.0 / (1.0 + jnp.exp(-small[:, 0:1])))
            flipped = small.T
            x = flipped[0:8, :]
            soft = jnp.maximum(x, 0.0) + jnp.log1p(jnp.exp(-jnp.abs(x)))
            steps = extra_ref[pl.ds(start + b, 1), :] - speed * soft[1:2, :]
            cum_row = lax.dot_general(
                jnp.broadcast_to(steps, (8, BLOCK)), upper, NN, preferred_element_type=F32, precision=lax.Precision.HIGHEST
            )[0:1, :]
            across = jnp.broadcast_to(cum_row, (BLOCK, BLOCK))
            down = across.T
            total = jnp.broadcast_to(cum_row[:, BLOCK - 1 : BLOCK], (BLOCK, BLOCK))
            decay = jnp.exp(jnp.where(row >= col, down - across, -1e30))
            grow = jnp.exp(down)
            both = mm(jnp.concatenate([k, q], axis=0), k, NT)
            mats.append(jnp.where(row > col, both[:BLOCK] * decay * strength, 0.0))
            right = jnp.concatenate([v * strength, k * (grow * strength)], axis=1)
            keep.append((q * grow, both[BLOCK:] * decay, right, k * jnp.exp(total - down)))
            lasts[start + b] = jnp.exp(total[0:8, :])
        invs = invert_unit_lower(mats, row, col)
        for b in range(count):
            query_dec, scores, right, keys_dec = keep[b]
            solved = mm(invs[b], right)
            seen = mm(scores, solved)
            kept = mm(keys_dec, solved, TN)
            high[start + b, :, :HEAD] = kept[:, :HEAD]
            high[start + b, :, HEAD:] = seen[:, :HEAD]
            low[start + b, :HEAD, :] = (query_dec - seen[:, HEAD:]).astype(BF16)
            low[start + b, HEAD:, :] = kept[:, HEAD:].astype(BF16)
        return carry

    lax.fori_loop(0, 2, half, 0)
    maps = (row == col).astype(F32)
    memory = jnp.zeros((HEAD, HEAD), F32)
    for j in range(blocks):
        both = jnp.concatenate([maps, memory], axis=1).astype(BF16)
        out = mm(low[j], both)
        g_ref[j * BLOCK : (j + 1) * BLOCK, :] = out[:HEAD, :HEAD].astype(BF16)
        h_ref[j * BLOCK : (j + 1) * BLOCK, :] = out[:HEAD, HEAD:] + high[j, :, HEAD:]
        last = lasts[j, 0:1, :]
        maps = maps * last - out[HEAD:, :HEAD]
        memory = memory * last - out[HEAD:, HEAD:] + high[j, :, :HEAD]
    ab_ref[:, :HEAD] = maps.astype(BF16)
    ab_ref[:, HEAD:] = memory.astype(BF16)


def span_terms(scal, head, rows, query, key, value, strength, decay, extra):
    length, depth = rows.shape
    blocks = length // BLOCK
    width = 4 * HEAD
    chunks = 4
    smem = pl.BlockSpec(memory_space=pltpu.SMEM)
    vmem = pl.BlockSpec(memory_space=pltpu.VMEM)
    hbm = pl.BlockSpec(memory_space=pltpu.HBM)
    return pl.pallas_call(
        functools.partial(span_kernel, chunks),
        out_shape=(
            jax.ShapeDtypeStruct((length, HEAD), BF16),
            jax.ShapeDtypeStruct((length, HEAD), F32),
            jax.ShapeDtypeStruct((HEAD, 2 * HEAD), BF16),
        ),
        in_specs=[smem, smem, hbm, hbm, hbm, hbm, vmem, vmem, vmem],
        out_specs=(vmem, vmem, vmem),
        scratch_shapes=[
            pltpu.VMEM((length, depth), BF16),
            pltpu.VMEM((depth, width), BF16),
            pltpu.VMEM((length // 2, width), F32),
            pltpu.VMEM((blocks, 2 * HEAD, HEAD), BF16),
            pltpu.VMEM((blocks, HEAD, 2 * HEAD), F32),
            pltpu.VMEM((blocks, 8, HEAD), F32),
            pltpu.SemaphoreType.DMA((3 + chunks,)),
        ],
        compiler_params=pltpu.CompilerParams(vmem_limit_bytes=SPAN_LIMIT * 1024 * 1024),
        cost_estimate=pl.CostEstimate(
            flops=length * 2 * (depth * width + 40 * HEAD * HEAD * 4),
            bytes_accessed=2 * (rows.size + depth * width) + length * HEAD * 6,
            transcendentals=0,
        ),
    )(scal, head, *[pltpu.with_memory_space_constraint(x, pltpu.HBM) for x in (rows, query, key, value)], strength, decay, extra)


def row_kernel(here_ref, own_ref, one_ref, two_ref, three_ref, before_ref, total_ref, slots):
    here = here_ref[0]
    slots[here] = own_ref[...]
    slots[(here + 3) % 4] = one_ref[...]
    slots[(here + 2) % 4] = two_ref[...]
    slots[(here + 1) % 4] = three_ref[...]
    row = lax.broadcasted_iota(jnp.int32, (HEAD, 2 * HEAD), 0)
    col = lax.broadcasted_iota(jnp.int32, (HEAD, 2 * HEAD), 1)
    eye = (row == col).astype(F32)
    so_far = slots[0].astype(F32)
    before = jnp.where(here == 0, eye, so_far)
    for k in range(1, 4):
        piece = slots[k]
        own = jnp.where(col >= HEAD, piece.astype(F32), 0.0)
        so_far = mm(piece[:, :HEAD], so_far) + own
        if k < 3:
            before = jnp.where(here > k, so_far, before)
    before_ref[...] = before
    total_ref[...] = so_far.astype(BF16)


def compose_row(here, own, one, two, three):
    vmem = pl.BlockSpec(memory_space=pltpu.VMEM)
    return pl.pallas_call(
        row_kernel,
        out_shape=(jax.ShapeDtypeStruct((HEAD, 2 * HEAD), F32), jax.ShapeDtypeStruct((HEAD, 2 * HEAD), BF16)),
        in_specs=[pl.BlockSpec(memory_space=pltpu.SMEM)] + [vmem] * 4,
        out_specs=(vmem, vmem),
        scratch_shapes=[pltpu.VMEM((4, HEAD, 2 * HEAD), BF16)],
        compiler_params=pltpu.CompilerParams(vmem_limit_bytes=8 * 1024 * 1024),
        cost_estimate=pl.CostEstimate(flops=12 * HEAD**3, bytes_accessed=8 * HEAD * HEAD, transcendentals=0),
    )(here, own, one, two, three)


def apply_kernel(here_ref, one_ref, two_ref, three_ref, before_ref, g_ref, h_ref, gain_ref, out_ref, slots):
    here = here_ref[0]
    slots[(here + 3) % 4] = one_ref[...]
    slots[(here + 2) % 4] = two_ref[...]
    slots[(here + 1) % 4] = three_ref[...]
    memory = jnp.where(here > 0, slots[0][:, HEAD:].astype(F32), 0.0)
    for k in range(1, 3):
        piece = slots[k]
        moved = mm(piece[:, :HEAD], memory) + piece[:, HEAD:].astype(F32)
        memory = jnp.where(here > k, moved, memory)
    memory = mm(before_ref[:, :HEAD], memory) + before_ref[:, HEAD:]
    heads_out = mm(g_ref[...], memory) + h_ref[...]
    scale = lax.rsqrt(jnp.mean(heads_out * heads_out, axis=1, keepdims=True) + norm_eps)
    out_ref[...] = (heads_out * scale * gain_ref[...]).astype(BF16)


def apply_memory(here, one, two, three, before, g, h, gain):
    vmem = pl.BlockSpec(memory_space=pltpu.VMEM)
    return pl.pallas_call(
        apply_kernel,
        out_shape=jax.ShapeDtypeStruct(h.shape, BF16),
        in_specs=[pl.BlockSpec(memory_space=pltpu.SMEM)] + [vmem] * 7,
        out_specs=vmem,
        scratch_shapes=[pltpu.VMEM((4, HEAD, 2 * HEAD), BF16)],
        compiler_params=pltpu.CompilerParams(vmem_limit_bytes=8 * 1024 * 1024),
        cost_estimate=pl.CostEstimate(flops=h.size * 2 * HEAD, bytes_accessed=h.size * 8, transcendentals=0),
    )(here, one, two, three, before, g, h, gain.reshape(1, HEAD))


def sum_kernel(*refs):
    total = refs[0][...].astype(F32)
    for ref in refs[1:-1]:
        total = total + ref[...].astype(F32)
    refs[-1][...] = total.astype(BF16)


def sum_parts(parts):
    vmem = pl.BlockSpec(memory_space=pltpu.VMEM)
    return pl.pallas_call(
        sum_kernel,
        out_shape=jax.ShapeDtypeStruct(parts[0].shape, BF16),
        in_specs=[vmem] * len(parts),
        out_specs=vmem,
        compiler_params=pltpu.CompilerParams(vmem_limit_bytes=4 * 1024 * 1024),
        cost_estimate=pl.CostEstimate(flops=10**6, bytes_accessed=2 * 9 * parts[0].size, transcendentals=0),
    )(*parts)


def output_kernel(chunks, core_ref, x_ref, w_ref, mine_ref, theirs_ref, weights, total, sems):
    tall = w_ref.shape[0] // chunks
    copies = [
        pltpu.make_async_copy(w_ref.at[pl.ds(i * tall, tall)], weights.at[pl.ds(i * tall, tall)], sems.at[i])
        for i in range(chunks)
    ]
    for copy in copies:
        copy.start()
    heads = tall // HEAD
    core = core_ref[0]
    owners = [pl.ds(pl.multiple_of(owner * BLOCK, BLOCK), BLOCK) for owner in (core, 1 - core)]
    for i, copy in enumerate(copies):
        rows = jnp.concatenate(
            [jnp.concatenate([x_ref[i * heads + h, at, :] for h in range(heads)], axis=1) for at in owners], axis=0
        )
        copy.wait()
        part = mm(rows, weights[i * tall : (i + 1) * tall, :])
        if i == 0:
            total[...] = part
        elif i < chunks - 1:
            total[...] += part
        else:
            whole = total[...] + part
            mine_ref[...] = whole[:BLOCK]
            theirs_ref[...] = whole[BLOCK:].astype(BF16)


def output_product(core, by_head, weights):
    depth, width = weights.shape
    count = by_head.shape[1]
    chunks = 4
    vmem = pl.BlockSpec(memory_space=pltpu.VMEM)
    return pl.pallas_call(
        functools.partial(output_kernel, chunks),
        out_shape=(jax.ShapeDtypeStruct((BLOCK, width), F32), jax.ShapeDtypeStruct((BLOCK, width), BF16)),
        in_specs=[pl.BlockSpec(memory_space=pltpu.SMEM), vmem, pl.BlockSpec(memory_space=pltpu.HBM)],
        out_specs=(vmem, vmem),
        scratch_shapes=[
            pltpu.VMEM((depth, width), BF16),
            pltpu.VMEM((count, width), F32),
            pltpu.SemaphoreType.DMA((chunks,)),
        ],
        cost_estimate=pl.CostEstimate(
            flops=2 * count * depth * width, bytes_accessed=2 * depth * width, transcendentals=0
        ),
        compiler_params=pltpu.CompilerParams(vmem_limit_bytes=32 * 1024 * 1024),
    )(core, by_head, pltpu.with_memory_space_constraint(weights, pltpu.HBM))


def join_kernel(mine_ref, theirs_ref, out_ref):
    out_ref[...] = (mine_ref[...].astype(F32) + theirs_ref[...].astype(F32)).astype(BF16)


def join_halves(mine, theirs):
    vmem = pl.BlockSpec(memory_space=pltpu.VMEM)
    return pl.pallas_call(
        join_kernel,
        out_shape=jax.ShapeDtypeStruct(mine.shape, BF16),
        in_specs=[vmem, vmem],
        out_specs=vmem,
        compiler_params=pltpu.CompilerParams(vmem_limit_bytes=8 * 1024 * 1024),
        cost_estimate=pl.CostEstimate(flops=10**6, bytes_accessed=8 * mine.size, transcendentals=0),
    )(mine, theirs)


def route_columns(side, experts):
    tokens = side.shape[1]
    expert = lax.broadcasted_iota(jnp.int32, (experts, tokens), 0).astype(F32)
    first, second = side[0:1] == expert, side[1:2] == expert
    named = (first | second).astype(F32)
    row = lax.broadcasted_iota(jnp.int32, (tokens, tokens), 0)
    col = lax.broadcasted_iota(jnp.int32, (tokens, tokens), 1)
    earlier = ((row < col) & (row // TOKENS == col // TOKENS)).astype(F32)
    return first, named, mm(named, earlier)


def slot_rows(named, slots, e):
    tokens = named.shape[1]
    rows = tokens // TOKENS * SLOTS
    row = lax.broadcasted_iota(jnp.int32, (rows, tokens), 0)
    col = lax.broadcasted_iota(jnp.int32, (rows, tokens), 1)
    taken = jnp.where(named[e : e + 1] > 0.5, slots[e : e + 1], -1.0)
    return (taken == (row % SLOTS).astype(F32)) & (row // SLOTS == col // TOKENS)


def pack_kernel(experts, tok_ref, out_ref):
    width = out_ref.shape[1]
    side = tok_ref[:, width:].astype(F32).T
    _, named, slots = route_columns(side, experts)
    rows = out_ref.shape[0] // experts
    group = 4
    for e in range(0, experts, group):
        pick = jnp.concatenate([slot_rows(named, slots, e + i).astype(F32) for i in range(group)], axis=0)
        out_ref[e * rows : (e + group) * rows, :] = mm(pick, tok_ref[:, :width]).astype(BF16)


def pack_tokens(tokens, experts):
    count, width = tokens.shape
    vmem = pl.BlockSpec(memory_space=pltpu.VMEM)
    rows = count // TOKENS * SLOTS * experts
    return pl.pallas_call(
        functools.partial(pack_kernel, experts),
        out_shape=jax.ShapeDtypeStruct((rows, width - HEAD), BF16),
        in_specs=[vmem],
        out_specs=vmem,
        cost_estimate=pl.CostEstimate(flops=2 * rows * count * width, bytes_accessed=2 * rows * width, transcendentals=0),
    )(tokens)


def combine_kernel(experts, devices, here_ref, side_ref, back_ref, *refs):
    out_refs, total = refs[:devices], refs[devices]
    side = side_ref[...].astype(F32).T
    first, named, slots = route_columns(side, experts)
    share = [side[2 + k : 3 + k] + side[4 + k : 5 + k] + side[6 + k : 7 + k] for k in range(2)]
    picks = []
    for e in range(experts):
        share_row = jnp.where(first[e : e + 1], share[0], share[1])
        picks.append(jnp.where(slot_rows(named, slots, e), share_row, 0.0))
    pick = jnp.concatenate(picks, axis=0)
    high = pick.astype(BF16)
    low = (pick - high.astype(F32)).astype(BF16)
    back = back_ref[...]
    total[...] = (mm(high, back, TN) + mm(low, back, TN)).reshape(total.shape)
    for k, out_ref in enumerate(out_refs):
        out_ref[...] = total[(here_ref[0] + k) % len(out_refs)].astype(BF16)


def combine_tokens(here, tokens, back, experts):
    count, _ = tokens.shape
    width = back.shape[1]
    devices = count // TOKENS
    piece = (TOKENS, width)
    return pl.pallas_call(
        functools.partial(combine_kernel, experts, devices),
        grid=(1,),
        out_shape=[jax.ShapeDtypeStruct(piece, BF16)] * devices,
        in_specs=[
            pl.BlockSpec(memory_space=pltpu.SMEM),
            pl.BlockSpec((count, HEAD), lambda i: (0, width // HEAD)),
            pl.BlockSpec(back.shape, lambda i: (0, 0)),
        ],
        out_specs=[pl.BlockSpec(piece, lambda i: (0, 0))] * devices,
        scratch_shapes=[pltpu.VMEM((devices, *piece), F32)],
        compiler_params=pltpu.CompilerParams(vmem_limit_bytes=24 * 1024 * 1024),
        cost_estimate=pl.CostEstimate(
            flops=4 * count * back.size, bytes_accessed=2 * back.size + 2 * count * width, transcendentals=0
        ),
    )(here, tokens, back)


def expert_kernel(own_ref, other_ref, gate_ref, up_ref, down_ref, mine_ref, theirs_ref, rows, gate, up, down, sems):
    half = own_ref.shape[0]
    pairs = (
        (own_ref, rows.at[pl.ds(0, half)]),
        (other_ref, rows.at[pl.ds(half, half)]),
        (gate_ref, gate),
        (up_ref, up),
        (down_ref, down),
    )
    copies = [pltpu.make_async_copy(src, dst, sems.at[i]) for i, (src, dst) in enumerate(pairs)]
    for copy in copies:
        copy.start()
    for copy in copies[:3]:
        copy.wait()
    gated = silu(mm(rows[...], gate[...], NT))
    copies[3].wait()
    hidden = (gated * mm(rows[...], up[...], NT)).astype(BF16)
    copies[4].wait()
    theirs_ref[...] = mm(hidden[half:], down[...]).astype(BF16)
    mine_ref[...] = mm(hidden[:half], down[...]).astype(BF16)


def expert_sums(own, other, gate, up, down):
    half, width = own.shape
    units = gate.shape[0]
    out = jax.ShapeDtypeStruct((half, width), BF16)
    vmem = pl.BlockSpec(memory_space=pltpu.VMEM)
    return pl.pallas_call(
        expert_kernel,
        out_shape=(out, out),
        in_specs=[pl.BlockSpec(memory_space=pl.ANY)] * 5,
        out_specs=(vmem, vmem),
        scratch_shapes=[
            pltpu.VMEM((2 * half, width), BF16),
            pltpu.VMEM((units, width), BF16),
            pltpu.VMEM((units, width), BF16),
            pltpu.VMEM((units, width), BF16),
            pltpu.SemaphoreType.DMA((5,)),
        ],
        cost_estimate=pl.CostEstimate(
            flops=12 * half * width * units, bytes_accessed=6 * units * width + 8 * half * width, transcendentals=0
        ),
        compiler_params=pltpu.CompilerParams(vmem_limit_bytes=36 * 1024 * 1024),
    )(own, other, *[pltpu.with_memory_space_constraint(x, pltpu.HBM) for x in (gate, up, down)])


def around(x, axis):
    size = lax.axis_size(axis)
    out = []
    for k in range(1, size):
        out.append(lax.ppermute(x, axis, [(i, (i + k) % size) for i in range(size)]))
    return out


def mixed_step(
    mixer_input_rows,
    mixer_norm_gain,
    query_weight,
    key_weight,
    value_weight,
    write_strength_projection,
    decay_projection,
    head_decay_speed,
    largest_write_strength,
    extra_log_decay,
    head_norm_gain,
    mixer_output_weight,
    expert_input_rows,
    expert_norm_gain,
    routes,
    expert_route_weight,
    gate_weight,
    up_weight,
    down_weight,
):
    head = lax.axis_index(TP)
    core = lax.axis_index("tp_1")
    experts = gate_weight.shape[0] * lax.axis_size(EP)
    cross = lambda x: lax.ppermute(x, "tp_1", [(0, 1), (1, 0)])

    mix_normed = rms_scale(mixer_input_rows, mixer_norm_gain)
    mix_rows = lax.all_gather(mix_normed, TP, axis=0, tiled=True)

    exp_normed = rms_scale(expert_input_rows, expert_norm_gain)
    parts, rest = [], expert_route_weight
    for _ in range(3):
        part = lax.reduce_precision(rest, 8, 7)
        parts.append(part.astype(BF16))
        rest = rest - part
    side = jnp.concatenate([routes.astype(BF16)] + parts, axis=1)
    side = jnp.pad(side, ((0, 0), (0, HEAD - side.shape[1])))
    own = jnp.concatenate([exp_normed, side], axis=1)
    copies = jnp.broadcast_to(own, (lax.axis_size("tp_0"), *own.shape))
    tokens = lax.all_to_all(copies, "tp_0", split_axis=0, concat_axis=0, tiled=True).reshape(-1, own.shape[1])
    packed = pack_tokens(tokens, experts)
    exp_rows = lax.all_to_all(packed, EP, split_axis=0, concat_axis=0, tiled=True)
    other_rows = cross(exp_rows)
    mine, theirs = expert_sums(exp_rows, other_rows, gate_weight[0].T, up_weight[0].T, down_weight[0])
    pair = join_halves(mine, cross(theirs))
    back = lax.all_to_all(pair, EP, split_axis=0, concat_axis=0, tiled=True)
    parts = combine_tokens(lax.axis_index("tp_0")[None], tokens, back, experts)

    scal = jnp.concatenate([head_decay_speed, largest_write_strength])
    extra = extra_log_decay.reshape(-1, BLOCK)
    gains, local, span = span_terms(
        scal,
        head[None],
        mix_rows,
        query_weight,
        key_weight,
        value_weight,
        write_strength_projection.T,
        decay_projection.T,
        extra,
    )
    row_pieces = around(span, "ep_1")
    before, total = compose_row(lax.axis_index("ep_1")[None], span, *row_pieces)
    mixed = apply_memory(lax.axis_index("ep_0")[None], *around(total, "ep_0"), before, gains, local, head_norm_gain)

    ring = lax.axis_size("tp_0")
    by_head = lax.all_to_all(
        mixed.reshape(ring, 2 * BLOCK, HEAD), "tp_0", split_axis=0, concat_axis=0, tiled=True
    )
    w_own = lax.all_gather(mixer_output_weight, "tp_0", axis=0, tiled=True)
    mix_mine, mix_theirs = output_product(core[None], by_head, w_own)
    mix_crossed = cross(mix_theirs)
    mix_out = join_halves(mix_mine, mix_crossed)

    arrived = [parts[0]]
    for k in range(1, ring):
        arrived.append(lax.ppermute(parts[k], "tp_0", [(i, (i + k) % ring) for i in range(ring)]))
    exp_out = sum_parts(arrived)
    return (mix_out, exp_out)


def solution(mesh):
    torus = Mesh(mesh.devices.reshape(4, 4, 8, 2), ("ep_0", "ep_1", "tp_0", "tp_1"))
    placed = (
        P(EP_TP, None),
        P(),
        P(None, TP),
        P(None, TP),
        P(None, TP),
        P(),
        P(),
        P(TP),
        P(TP),
        P(EP, TP),
        P(),
        P(TP, None),
        P(EP_TP, None),
        P(),
        P(EP_TP, None),
        P(EP_TP, None),
        P(EP, None, TP),
        P(EP, None, TP),
        P(EP, TP, None),
    )
    return jax.shard_map(
        mixed_step,
        mesh=torus,
        in_specs=placed,
        out_specs=(P(EP_TP, None), P(EP_TP, None)),
        check_vma=False,
    )
```
